32 devices in a mesh: ep: 8 (over z, core), tp: 4 (over y, x).
Axes of the slice: x: 2, y: 2, z: 4, core: 2. Of those that a mesh axis runs over, the one named last changes fastest.
Arguments:
- queries: bfloat16 [1024, 1536], P('ep', 'tp'), may hold values from -64 to 64
- kv_latent: bfloat16 [1024, 512], P('ep'), may hold values from -60 to 60
- rope_key: bfloat16 [1024, 32], P('ep'), may hold values from -64 to 64
- latent_gain: float32 [512], replicated, may hold values from 0.1 to 1.9
- key_up: bfloat16 [512, 1024], P(None, 'tp'), may hold values from -0.25 to 0.25
- value_up: bfloat16 [512, 1024], P(None, 'tp'), may hold values from -40 to 40
- query_gain: float32 [96], replicated, may hold values from 0.3 to 4
- key_gain: float32 [96], replicated, may hold values from 0.3 to 4
- out_gain: float32 [1024], replicated, may hold values from 0.1 to 1.9
- out_proj: bfloat16 [1024, 4096], P(None, 'tp'), may hold values from -0.1875 to 0.1875
- moe_input: bfloat16 [1024, 4096], P('ep'), may hold values from -60 to 60
- moe_gain: float32 [4096], replicated, may hold values from 0.1 to 1.9
- expert_ids: int32 [1024, 2], P('ep'), may hold values from 0 to 31, as said below
- route_weights: float32 [1024, 2], P('ep'), may hold values from 0.2 to 1
- w_gate: bfloat16 [32, 4096, 2048], P('ep', None, 'tp'), may hold values from -0.09375 to 0.09375
- w_up: bfloat16 [32, 4096, 2048], P('ep', None, 'tp'), may hold values from -0.09375 to 0.09375
- w_down: bfloat16 [32, 2048, 4096], P('ep', 'tp'), may hold values from -0.125 to 0.125
Outputs:
- mixed: bfloat16 [1024, 4096], P('ep', 'tp')
- expert_out: bfloat16 [1024, 4096], P('ep', 'tp')
The draws below stay inside these ranges and needn't reach their ends.
Inputs may be any that keep to these rules, and one draw needn't show every extreme that they name: `expert_ids`: both experts of a row lie in one group (g * 8 to g * 8 + 7) and differ. In each aligned block of 128 rows no expert is named more than 12 times, and some expert is named exactly 12 times.
All inputs are finite; a program needn't handle non-finite values.
Results may differ from the reference program's by a relative error of at most 0.015.
The reference program's roundings to bfloat16 on the way count: a program that leaves them out, or rounds other values in their place, can miss the bound.
Values may be sent and summed in bfloat16 or wider, within the bound.
No kernel may reach another device: no remote copies, remote signals or barrier semaphores. Data moves between devices by JAX's collectives and lax.ppermute only.
A program may use at most 128 MiB of HBM per device.

```python
import jax
import jax.numpy as jnp
from jax import lax

D = 4096
HEADS = 16
NOPE = 64
ROPE = 32
VDIM = 64
KV_RANK = 512
PER_GROUP = 8
D_EXP = 2048
TOP = 2
TOK_DEV = 128
QKD = 96
EXPERTS = 32
TOKENS = 1024
CAP = 12
N_EP = 8
N_TP = 4


def draw_rope_key(key, part):
    drawn = jnp.clip(jax.random.normal(jax.random.fold_in(key, 21), (TOKENS, ROPE), jnp.float32), -6.0, 6.0)
    return drawn.astype(jnp.bfloat16)


def draw_queries(key, part):
    drawn = jnp.clip(jax.random.normal(jax.random.fold_in(key, 31), (TOKENS, HEADS, QKD), jnp.float32), -6.0, 6.0)
    return drawn.reshape(TOKENS, HEADS * QKD).astype(jnp.bfloat16)


def draw_query_gain(key, part):
    drawn = jax.random.uniform(jax.random.fold_in(key, 41), (QKD,), jnp.float32, 0.3, 1.7)
    return drawn


def draw_key_gain(key, part):
    drawn = jax.random.uniform(jax.random.fold_in(key, 51), (QKD,), jnp.float32, 0.3, 1.7)
    return drawn


def scaled_rows(key, salt, row_count, col_count):
    drawn = jnp.clip(jax.random.normal(jax.random.fold_in(key, salt), (row_count, col_count), jnp.float32), -6.0, 6.0)
    return drawn


def draw_kv_latent(key, part):
    return scaled_rows(key, 61, TOKENS, KV_RANK).astype(jnp.bfloat16)


def draw_moe_input(key, part):
    return scaled_rows(key, 71, TOKENS, D).astype(jnp.bfloat16)


def draw_value_up(key, part):
    drawn = jax.random.normal(jax.random.fold_in(key, 81), (KV_RANK, HEADS * VDIM), jnp.float32) * KV_RANK ** (-0.5)
    head_pos = (jnp.arange(HEADS * VDIM) // VDIM).astype(jnp.float32) / (HEADS - 1)
    scale = 3.0 ** head_pos
    return jnp.clip(drawn * scale[None, :], -40.0, 40.0).astype(jnp.bfloat16)


def draw_expert_ids(key, part):
    block_keys = jax.random.split(jax.random.fold_in(key, 91), TOKENS // TOK_DEV)

    def one_block(block_key):
        parts_key = jax.random.split(block_key, 6)
        biggest = jax.random.randint(parts_key[0], (), 0, 4)
        low_count = TOK_DEV // 8
        high_count = TOK_DEV // 4
        count_a = jax.random.randint(parts_key[1], (), low_count, high_count + 1)
        count_b = jax.random.randint(parts_key[2], (), low_count, high_count + 1)
        count_c = 5 * TOK_DEV // 8 - count_a - count_b
        others = (biggest + 1 + jnp.arange(3)) % 4
        counts = jnp.zeros((4,), jnp.int32).at[biggest].set(3 * TOK_DEV // 8)
        counts = counts.at[others].set(jnp.stack([count_a, count_b, count_c]).astype(jnp.int32))
        ends = jnp.cumsum(counts)
        ranks = jnp.arange(TOK_DEV)
        group_of = jnp.sum((ranks[:, None] >= ends[None, :]).astype(jnp.int32), axis=1)
        within = ranks - (ends - counts)[group_of]
        shifts = jax.random.randint(parts_key[3], (4,), 0, PER_GROUP)
        steps_apart = jax.random.randint(parts_key[4], (4,), 1, PER_GROUP)
        first_pick = (shifts[group_of] + within) % PER_GROUP
        second_pick = (shifts[group_of] + within + steps_apart[group_of]) % PER_GROUP
        chosen = jnp.stack([first_pick, second_pick], axis=1) + group_of[:, None] * PER_GROUP
        order = jax.random.permutation(parts_key[5], TOK_DEV)
        return chosen[order]
    return jax.vmap(one_block)(block_keys).reshape(TOKENS, 2).astype(jnp.int32)


def block_levels(own_key, shape, cuts, low, largest):
    factor_of, own = 1.0, jax.random.fold_in(own_key, 6)
    for dim, blocks in cuts:
        draws = jnp.exp(jax.random.uniform(jax.random.fold_in(own, dim), (blocks,), jnp.float32, low / len(cuts), largest / len(cuts)))
        factor_of = factor_of * jnp.repeat(draws, shape[dim] // blocks).reshape([-1 if axis == dim else 1 for axis in range(len(shape))])
    return factor_of


def noise(key, dims, deviation, most, cuts=(), kind=jnp.bfloat16):
    entries = jax.random.normal(key, dims, jnp.float32) * deviation
    if len(cuts) > 0:
        entries = block_levels(key, dims, cuts, -0.22, 0.18) * entries
    return jnp.clip(entries, min=-most, max=most).astype(kind)


def setup_inputs(seed: int = 0) -> dict:
    seeds = jax.random.split(jax.random.key(seed), 18)
    return {
        "queries": draw_queries(jax.random.fold_in(seeds[17], 71), 0),
        "kv_latent": draw_kv_latent(jax.random.fold_in(seeds[17], 71), 0),
        "rope_key": draw_rope_key(jax.random.fold_in(seeds[17], 71), 0),
        "latent_gain": jnp.clip(1.0 + 0.18 * jax.random.normal(seeds[3], (KV_RANK,), jnp.float32), 0.1, 1.9),
        "key_up": noise(seeds[4], (KV_RANK, HEADS * NOPE), KV_RANK ** -0.5, 0.25, ((1, 4),)),
        "value_up": draw_value_up(jax.random.fold_in(seeds[17], 71), 0),
        "query_gain": draw_query_gain(jax.random.fold_in(seeds[17], 71), 0),
        "key_gain": draw_key_gain(jax.random.fold_in(seeds[17], 71), 0),
        "out_gain": jnp.clip(1.0 + 0.18 * jax.random.normal(seeds[8], (HEADS * VDIM,), jnp.float32), 0.1, 1.9),
        "out_proj": noise(seeds[9], (HEADS * VDIM, D), (HEADS * VDIM) ** -0.5, 0.1875, ((1, 4),)),
        "moe_input": draw_moe_input(jax.random.fold_in(seeds[17], 71), 0),
        "moe_gain": jnp.clip(1.0 + 0.18 * jax.random.normal(seeds[11], (D,), jnp.float32), 0.1, 1.9),
        "expert_ids": draw_expert_ids(jax.random.fold_in(seeds[17], 71), 0),
        "route_weights": jnp.clip(0.2 + 0.8 * jax.random.uniform(seeds[13], (TOKENS, TOP), jnp.float32) ** block_levels(seeds[13], (TOKENS, TOP), ((0, 8),), -0.2, 0.2), 0.2, 1.0),
        "w_gate": noise(seeds[14], (EXPERTS, D, D_EXP), D ** -0.5, 0.09375, ((0, 8), (2, 4))),
        "w_up": noise(seeds[15], (EXPERTS, D, D_EXP), D ** -0.5, 0.09375, ((0, 8), (2, 4))),
        "w_down": noise(seeds[16], (EXPERTS, D_EXP, D), D_EXP ** -0.5, 0.125, ((0, 8), (1, 4))),
    }


EPS = 1e-06
THETA = 10000.0

def rotate_half(values_in, positions):
    half_width = ROPE // 2
    inverse = THETA ** (-jnp.arange(half_width, dtype=jnp.float32) / half_width)
    angles = positions.astype(jnp.float32)[:, None] * inverse
    cosine = jnp.cos(angles)[:, None, :]
    sine = jnp.sin(angles)[:, None, :]
    first_half = values_in[..., :half_width]
    second_half = values_in[..., half_width:]
    return jnp.concatenate([first_half * cosine - second_half * sine, second_half * cosine + first_half * sine], axis=-1)

def head_norm(values_in, gain_vec):
    return values_in * lax.rsqrt(lax.optimization_barrier(jnp.mean(values_in * values_in, axis=-1, keepdims=True)) + EPS) * gain_vec

def make_queries(queries, query_gain, positions):
    row_count = queries.shape[0]
    head_count = queries.shape[1] // QKD
    normed = head_norm(queries.astype(jnp.float32).reshape(row_count, head_count, QKD), query_gain)
    turned = jnp.concatenate([normed[..., :NOPE], rotate_half(normed[..., NOPE:], positions)], axis=-1)
    return turned.astype(jnp.bfloat16)

def make_keys(latent, rope_part, latent_gain, key_up, value_up, key_gain, positions):
    row_count = latent.shape[0]
    head_count = key_up.shape[1] // NOPE
    latent_f = latent.astype(jnp.float32)
    latent_n = (latent_f * lax.rsqrt(lax.optimization_barrier(jnp.mean(latent_f * latent_f, axis=-1, keepdims=True)) + EPS) * latent_gain).astype(jnp.bfloat16)
    key_nope = jnp.dot(latent_n, key_up, preferred_element_type=jnp.float32).astype(jnp.bfloat16)
    key_nope = lax.optimization_barrier(key_nope)
    value_rows = jnp.dot(latent_n, value_up, preferred_element_type=jnp.float32).astype(jnp.bfloat16)
    shared = jnp.broadcast_to(rope_part.astype(jnp.float32)[:, None, :], (row_count, head_count, ROPE))
    key_full = jnp.concatenate([key_nope.astype(jnp.float32).reshape(row_count, head_count, NOPE), shared], axis=-1)
    normed = head_norm(key_full, key_gain)
    turned = jnp.concatenate([normed[..., :NOPE], rotate_half(normed[..., NOPE:], positions)], axis=-1)
    return (turned.astype(jnp.bfloat16), value_rows.reshape(row_count, head_count, VDIM))

def attention(query_rot, key_rot, value_rows):
    block_rows = 512
    block_count = TOKENS // block_rows
    key_pos = jnp.arange(TOKENS)
    keys_f = key_rot.astype(jnp.float32)
    values_f = value_rows.astype(jnp.float32)
    head_count = query_rot.shape[1]

    def one_block(index):
        first = index * block_rows
        query_blk = lax.dynamic_slice_in_dim(query_rot, first, block_rows, 0).astype(jnp.float32)
        scores = jnp.einsum('qhd,khd->hqk', query_blk, keys_f) * QKD ** (-0.5)
        query_pos = first + jnp.arange(block_rows)
        visible = key_pos[None, :] <= query_pos[:, None]
        scores = jnp.where(visible[None], scores, -1e+30)
        top_score = lax.optimization_barrier(jnp.max(scores, axis=-1, keepdims=True))
        expo = jnp.exp(scores - top_score)
        probs = lax.optimization_barrier(expo.astype(jnp.bfloat16))
        totals = lax.optimization_barrier(jnp.sum(expo, axis=-1))
        weighted = jnp.einsum('hqk,khd->hqd', probs.astype(jnp.float32), values_f) / totals[..., None]
        return weighted.astype(jnp.bfloat16)
    outcome = lax.map(one_block, jnp.arange(block_count))
    return outcome.transpose(0, 2, 1, 3).reshape(TOKENS, head_count * VDIM)

def reference(queries, kv_latent, rope_key, latent_gain, key_up, value_up, query_gain, key_gain, out_gain, out_proj, moe_input, moe_gain, expert_ids, route_weights, w_gate, w_up, w_down):
    positions = jnp.arange(TOKENS, dtype=jnp.int32)
    query_rot = make_queries(queries, query_gain, positions)
    key_rot, value_rows = make_keys(kv_latent, rope_key, latent_gain, key_up, value_up, key_gain, positions)
    attn = attention(query_rot, key_rot, value_rows)
    attn_f = attn.astype(jnp.float32)
    inverse_rms = lax.rsqrt(lax.optimization_barrier(jnp.mean(attn_f * attn_f, axis=-1)) + EPS)
    attn_n = (attn_f * out_gain).astype(jnp.bfloat16)
    mixed = (jnp.dot(attn_n, out_proj, preferred_element_type=jnp.float32) * inverse_rms[:, None]).astype(jnp.bfloat16)
    stream_f = moe_input.astype(jnp.float32)
    normed = (stream_f * lax.rsqrt(lax.optimization_barrier(jnp.mean(stream_f * stream_f, axis=-1, keepdims=True)) + EPS) * moe_gain).astype(jnp.bfloat16)
    flat_ids = expert_ids.reshape(-1).astype(jnp.int32)
    pick_count = TOKENS * TOP
    onehot = (flat_ids[:, None] == jnp.arange(EXPERTS, dtype=jnp.int32)[None, :]).astype(jnp.int32)
    per_block = onehot.reshape(N_EP, TOK_DEV * TOP, EXPERTS)
    earlier = (jnp.cumsum(per_block, axis=1) - per_block).astype(jnp.int32)
    slot_rank = lax.optimization_barrier(jnp.sum(earlier * per_block, axis=-1)).reshape(-1).astype(jnp.int32)
    block_index = (jnp.arange(pick_count, dtype=jnp.int32) // (TOK_DEV * TOP)).astype(jnp.int32)
    slot_count = N_EP * CAP
    slot_index = (flat_ids * slot_count + block_index * CAP + slot_rank).astype(jnp.int32)
    token_index = (jnp.arange(pick_count, dtype=jnp.int32) // TOP).astype(jnp.int32)
    slot_token = jnp.zeros((EXPERTS * slot_count,), jnp.int32).at[slot_index].set(token_index)
    expert_rows = normed[slot_token].reshape(EXPERTS, slot_count, D)
    shard_width = D_EXP // N_TP

    def one_expert(operands):
        rows_in, gate_w, up_w, down_w = operands
        gate = jnp.dot(rows_in, gate_w, preferred_element_type=jnp.float32)
        upper = jnp.dot(rows_in, up_w, preferred_element_type=jnp.float32)
        act = (jax.nn.silu(gate) * upper).astype(jnp.bfloat16)
        partials = jnp.einsum('sjf,jfd->jsd', act.reshape(slot_count, N_TP, shard_width).astype(jnp.float32), down_w.reshape(N_TP, shard_width, D).astype(jnp.float32))
        partials = lax.optimization_barrier(partials.astype(jnp.bfloat16))
        return lax.optimization_barrier(jnp.sum(partials.astype(jnp.float32), axis=0)).astype(jnp.bfloat16)
    expert_y = lax.map(one_expert, (expert_rows, w_gate, w_up, w_down)).reshape(EXPERTS * slot_count, D)
    picked = expert_y[slot_index].reshape(TOKENS, TOP, D).astype(jnp.float32)
    expert_out = lax.optimization_barrier(jnp.sum(picked * route_weights[..., None], axis=1)).astype(jnp.bfloat16)
    return (mixed, expert_out)
```

```python
import functools

import jax
import jax.numpy as jnp
import numpy as np
from jax import lax
from jax.experimental import pallas as pl
from jax.experimental.pallas import tpu as pltpu
from jax.sharding import PartitionSpec as P

NOPE = 64
ROPE = 32
VDIM = 64
QKD = 96
CAP = 12
TOP = 2
PER_GROUP = 8


EPS = 1e-06
THETA = 10000.0


def rotate_half(values_in, positions):
    half_width = ROPE // 2
    inverse = THETA ** (-jnp.arange(half_width, dtype=jnp.float32) / half_width)
    angles = positions.astype(jnp.float32)[:, None] * inverse
    cosine = jnp.cos(angles)[:, None, :]
    sine = jnp.sin(angles)[:, None, :]
    first_half = values_in[..., :half_width]
    second_half = values_in[..., half_width:]
    return jnp.concatenate(
        [first_half * cosine - second_half * sine, second_half * cosine + first_half * sine],
        axis=-1,
    )


def head_norm(values_in, gain_vec):
    return (
        values_in
        * lax.rsqrt(jnp.mean(values_in * values_in, axis=-1, keepdims=True) + EPS)
        * gain_vec
    )


def make_queries(queries, query_gain, positions):
    row_count = queries.shape[0]
    head_count = queries.shape[1] // QKD
    normed = head_norm(queries.astype(jnp.float32).reshape(row_count, head_count, QKD), query_gain)
    turned = jnp.concatenate(
        [normed[..., :NOPE], rotate_half(normed[..., NOPE:], positions)], axis=-1
    )
    return turned.astype(jnp.bfloat16)


def make_keys(latent, rope_part, latent_gain, key_up, value_up, key_gain, positions):
    row_count = latent.shape[0]
    head_count = key_up.shape[1] // NOPE
    latent_f = latent.astype(jnp.float32)
    latent_n = (
        latent_f
        * lax.rsqrt(jnp.mean(latent_f * latent_f, axis=-1, keepdims=True) + EPS)
        * latent_gain
    ).astype(jnp.bfloat16)
    key_nope = jnp.dot(latent_n, key_up, preferred_element_type=jnp.float32).astype(jnp.bfloat16)
    key_nope = lax.optimization_barrier(key_nope)
    value_rows = jnp.dot(latent_n, value_up, preferred_element_type=jnp.float32).astype(
        jnp.bfloat16
    )
    shared = jnp.broadcast_to(
        rope_part.astype(jnp.float32)[:, None, :], (row_count, head_count, ROPE)
    )
    key_full = jnp.concatenate(
        [key_nope.astype(jnp.float32).reshape(row_count, head_count, NOPE), shared], axis=-1
    )
    normed = head_norm(key_full, key_gain)
    turned = jnp.concatenate(
        [normed[..., :NOPE], rotate_half(normed[..., NOPE:], positions)], axis=-1
    )
    return (turned.astype(jnp.bfloat16), value_rows.reshape(row_count, head_count, VDIM))


def shards(
    queries,
    kv_latent,
    rope_key,
    latent_gain,
    key_up,
    value_up,
    query_gain,
    key_gain,
    out_gain,
    out_proj,
    moe_input,
    moe_gain,
    expert_ids,
    route_weights,
    w_gate,
    w_up,
    w_down,
):
    tok_rows = queries.shape[0]
    head_count = key_up.shape[1] // NOPE
    query_pos = lax.axis_index("ep") * tok_rows + jnp.arange(tok_rows, dtype=jnp.int32)
    query_rot = make_queries(queries, query_gain, query_pos)
    inv_scale = QKD ** (-0.5)
    blocks_in = (
        lax.all_gather(kv_latent, "ep", axis=0, tiled=True),
        lax.all_gather(rope_key, "ep", axis=0, tiled=True),
    )
    key_pos = jnp.arange(blocks_in[0].shape[0], dtype=jnp.int32)
    key_rot, value_rows = make_keys(
        blocks_in[0], blocks_in[1], latent_gain, key_up, value_up, key_gain, key_pos
    )
    top_prev = jnp.full((head_count, tok_rows), -1e30, jnp.float32)
    key_pos = jnp.arange(key_rot.shape[0], dtype=jnp.int32)
    scores = (
        jnp.einsum("qhd,khd->hqk", query_rot, key_rot, preferred_element_type=jnp.float32)
        * inv_scale
    )
    visible = key_pos[None, :] <= query_pos[:, None]
    scores = jnp.where(visible[None], scores, -1e30)
    top_new = jnp.maximum(top_prev, jnp.max(scores, axis=-1))
    expo = jnp.exp(scores - top_new[..., None])
    total_new = jnp.sum(expo, axis=-1)
    accum_new = jnp.einsum(
        "hqk,khd->hqd", expo.astype(jnp.bfloat16), value_rows, preferred_element_type=jnp.float32
    )
    attn = (accum_new / total_new[..., None]).astype(jnp.bfloat16)
    attn = attn.transpose(1, 0, 2).reshape(tok_rows, head_count * VDIM)
    block_f = lax.all_gather(attn, "tp", axis=1, tiled=True).astype(jnp.float32)
    scaled = (block_f * out_gain[None, :]).astype(jnp.bfloat16)
    product = jnp.dot(scaled, out_proj, preferred_element_type=jnp.float32)
    product, squares = (product, jnp.sum(block_f * block_f, axis=-1))
    mixed = (product * lax.rsqrt(squares / out_gain.shape[0] + EPS)[:, None]).astype(jnp.bfloat16)
    row_count = moe_input.shape[0]
    top_count = expert_ids.shape[1]
    local_experts = w_gate.shape[0]
    ep_count = lax.axis_size("ep")
    expert_count = local_experts * ep_count
    stream_f = moe_input.astype(jnp.float32)
    normed = (
        stream_f * lax.rsqrt(jnp.mean(stream_f * stream_f, axis=-1, keepdims=True) + EPS) * moe_gain
    ).astype(jnp.bfloat16)
    flat_ids = expert_ids.reshape(-1)
    onehot = (flat_ids[:, None] == jnp.arange(expert_count, dtype=jnp.int32)[None, :]).astype(
        jnp.int32
    )
    slot_rank = jnp.sum((jnp.cumsum(onehot, axis=0) - onehot) * onehot, axis=1)
    slot_index = flat_ids * CAP + slot_rank
    token_index = jnp.arange(row_count * top_count, dtype=jnp.int32) // top_count
    slot_token = jnp.zeros((expert_count * CAP,), jnp.int32).at[slot_index].set(token_index)
    slot_used = jnp.zeros((expert_count * CAP,), jnp.bool_).at[slot_index].set(True)
    outgoing = jnp.where(slot_used[:, None], normed[slot_token], jnp.zeros((), jnp.bfloat16))
    outgoing = outgoing.reshape(ep_count, local_experts, CAP, normed.shape[1])
    piece_width = normed.shape[1] // lax.axis_size("tp")
    my_columns = lax.dynamic_slice_in_dim(
        outgoing, lax.axis_index("tp") * piece_width, piece_width, 3
    )
    arrived_part = lax.all_to_all(my_columns, "ep", split_axis=0, concat_axis=0, tiled=True)
    piece = lax.all_gather(arrived_part, "tp", axis=3, tiled=True)
    gate_acc = jnp.einsum("secd,edf->secf", piece, w_gate, preferred_element_type=jnp.float32)
    upper_acc = jnp.einsum("secd,edf->secf", piece, w_up, preferred_element_type=jnp.float32)
    hidden = (jax.nn.silu(gate_acc) * upper_acc).astype(jnp.bfloat16)
    out_cols = w_down.shape[2] // lax.axis_size("tp")
    term = jnp.einsum("secf,efd->dsec", hidden, w_down, preferred_element_type=jnp.float32)
    summed = lax.psum_scatter(
        term.reshape(lax.axis_size("tp") * out_cols, -1).astype(jnp.bfloat16),
        "tp",
        scatter_dimension=0,
        tiled=True,
    )
    expert_y = summed.T.reshape(ep_count, local_experts * CAP, out_cols)
    returned_rows = lax.all_to_all(expert_y, "ep", split_axis=0, concat_axis=0, tiled=True).reshape(
        expert_count * CAP, out_cols
    )
    picked = returned_rows[slot_index].reshape(row_count, top_count, out_cols).astype(jnp.float32)
    expert_out = jnp.sum(picked * route_weights[..., None], axis=1).astype(jnp.bfloat16)
    return (mixed, expert_out)


BF16 = jnp.bfloat16
F32 = jnp.float32
ANY = pl.BlockSpec(memory_space=pl.ANY)
WHOLE = pl.BlockSpec(memory_space=pltpu.VMEM)
SCALARS = pl.BlockSpec(memory_space=pltpu.SMEM)
META = 128


def iota(shape, dim):
    return lax.broadcasted_iota(jnp.int32, shape, dim)


def dot(left, right):
    return jnp.dot(left, right, preferred_element_type=F32)


def dot_nt(left, right):
    return lax.dot_general(left, right, (((1,), (1,)), ((), ())), preferred_element_type=F32)


def one_if(condition):
    return jnp.where(condition, 1.0, 0.0).astype(BF16)


def cost(flops, in_bytes):
    return pl.CostEstimate(flops=int(flops), bytes_accessed=int(in_bytes), transcendentals=0)


def limits(mib):
    return pltpu.CompilerParams(vmem_limit_bytes=mib * 1024 * 1024)


def dispatch_kernel(chips, experts, slots, info, x_ref, gain_ref, ids_ref, route_ref, *outs):
    rows = x_ref.shape[0]
    width = outs[chips].shape[1]
    sources, diagonals, pick_ref = outs[:chips], outs[chips : 2 * chips], outs[2 * chips]
    stream = x_ref[...].astype(F32)
    inverse = lax.rsqrt(jnp.mean(stream * stream, axis=-1, keepdims=True) + EPS)
    ids = ids_ref[...]
    first, second = ids[:, 0:1], ids[:, 1:2]
    group = lax.shift_right_logical(first, jnp.int32(PER_GROUP.bit_length() - 1))
    target = group - info[2]
    target = jnp.where(target < 0, target + chips, target)
    lanes = iota((rows, META), 1)
    hot_first, hot_second = lanes == first, lanes == second
    hot_target = lanes == target + experts
    earlier = one_if(iota((rows, rows), 1) < iota((rows, rows), 0))
    counts = dot(earlier, one_if(hot_first | hot_second | hot_target))

    def at(mask):
        return jnp.sum(jnp.where(mask, counts, 0.0), axis=-1, keepdims=True)

    slot = target.astype(F32) * slots + at(hot_target)
    values = [(first - group * PER_GROUP + 1).astype(F32), at(hot_first)]
    values += [(second - group * PER_GROUP + 1).astype(F32), at(hot_second)]
    for k in range(TOP):
        weight = route_ref[:, k : k + 1]
        high = weight.astype(BF16).astype(F32)
        middle = (weight - high).astype(BF16).astype(F32)
        values += [high, middle, weight - high - middle]
    meta = jnp.zeros((rows, META), F32)
    for lane, value in enumerate(values):
        meta = jnp.where(lanes == lane, value, meta)
    pick_ref[...] = one_if(iota((rows, chips * slots), 1).astype(F32) == slot)
    on_diagonal = iota((rows, rows), 0) == iota((rows, rows), 1)
    slot_row = jnp.sum(jnp.where(on_diagonal, slot, 0.0), axis=0, keepdims=True)
    select = one_if(iota((chips * slots, rows), 0).astype(F32) == slot_row)
    meta_rows = dot(select, meta.astype(BF16)).astype(BF16)
    for which, refs in ((0, sources), (3, diagonals)):
        columns = pl.ds(pl.multiple_of((info[0] ^ which) * width, 128), width)
        part = x_ref[:, columns].astype(F32) * inverse * gain_ref[:, columns]
        picked = dot(select, part.astype(BF16)).astype(BF16)
        for k in range(chips):
            refs[k][:, :width] = picked[k * slots : (k + 1) * slots]
    for k in range(chips):
        sources[k][:, width:] = meta_rows[k * slots : (k + 1) * slots]


def make_dispatch(info, moe_input, moe_gain, expert_ids, route_weights, chips, experts, slots, width):
    rows = moe_input.shape[0]
    shapes = [jax.ShapeDtypeStruct((slots, width + META), BF16)] * chips
    shapes += [jax.ShapeDtypeStruct((slots, width), BF16)] * chips
    shapes += [jax.ShapeDtypeStruct((rows, chips * slots), BF16)]
    outs = pl.pallas_call(
        functools.partial(dispatch_kernel, chips, experts, slots),
        out_shape=shapes,
        in_specs=[SCALARS] + [WHOLE] * 4,
        out_specs=[WHOLE] * len(shapes),
        compiler_params=limits(16),
        cost_estimate=cost(2e9, 4e6),
        name="dispatch",
    )(info, moe_input, moe_gain[None], expert_ids, route_weights)
    return outs[:chips], outs[chips : 2 * chips], outs[2 * chips]


def first_kernel(chips, slots, local, info, xm, xt, mm, mt, wg, wu, acc, sel, back, weight):
    index = pl.program_id(0)
    per_block, half = 2 * chips * CAP, chips * slots

    @pl.when(index == 0)
    def _():
        core = info[1].astype(F32)
        unit = one_if(iota((16, META), 0) == iota((16, META), 1))
        total = jnp.zeros((local * per_block, 1), F32)
        for side, meta_ref in ((0, mm), (1, mt)):
            meta = meta_ref[...]
            turned = dot_nt(unit, meta)
            cols = meta.astype(F32)

            def slot_of(take, block, k):
                expert = take(2 * k) - 1.0 - core * local
                inside = (expert >= 0.0) & (expert < local)
                return jnp.where(inside, expert * per_block + block * CAP + take(2 * k + 1), -1.0)

            def block_of(shape, dim):
                place = iota(shape, dim)
                block = jnp.full(shape, side * chips, jnp.int32)
                for k in range(1, chips):
                    block = block + jnp.where(place >= k * slots, 1, 0)
                return block.astype(F32)

            def row_value(k):
                return turned[k : k + 1, :]

            def col_value(k):
                return cols[:, k : k + 1]

            places = iota((local * per_block, half), 0).astype(F32)
            hits = [places == slot_of(row_value, block_of((1, half), 1), k) for k in range(TOP)]
            for k in range(TOP):
                base = 2 * TOP + 3 * k
                share = row_value(base) + row_value(base + 1) + row_value(base + 2)
                total += jnp.sum(jnp.where(hits[k], share, 0.0), axis=-1, keepdims=True)
            sel[side] = one_if(hits[0] | hits[1])
            wanted = [slot_of(col_value, block_of((half, 1), 0), k) for k in range(TOP)]
            lanes = iota((half, META), 1)
            for e in range(local):
                spot = (lanes + e * per_block).astype(F32)
                own = lanes < per_block
                back[side, e] = one_if(own & ((spot == wanted[0]) | (spot == wanted[1])))
        weight[...] = jnp.broadcast_to(total, weight.shape)

    mine = pl.ds(pl.multiple_of(index * per_block, 16), per_block)
    rows = (dot(sel[0, mine, :], xm[...]) + dot(sel[1, mine, :], xt[...])).astype(BF16)
    hidden = wg.shape[2]
    acc[0, :, :hidden] = dot(rows, wg[0])
    acc[0, :, hidden:] = dot(rows, wu[0])


def first_quarter(info, xm, xt, mm, mt, w_gate, w_up, chips, slots):
    local, hidden, width = w_gate.shape[0], w_gate.shape[2], xm.shape[1]
    per_block, half = 2 * chips * CAP, chips * slots
    shapes = [
        jax.ShapeDtypeStruct((local, per_block, 2 * hidden), F32),
        jax.ShapeDtypeStruct((2, local * per_block, half), BF16),
        jax.ShapeDtypeStruct((2, local, half, META), BF16),
        jax.ShapeDtypeStruct((local * per_block, META), F32),
    ]
    weights = pl.BlockSpec((1, width, hidden), lambda e, info: (e, info[0], 0))
    return pl.pallas_call(
        functools.partial(first_kernel, chips, slots, local),
        out_shape=shapes,
        grid_spec=pltpu.PrefetchScalarGridSpec(
            num_scalar_prefetch=1,
            grid=(local,),
            in_specs=[WHOLE] * 4 + [weights] * 2,
            out_specs=[pl.BlockSpec((1, per_block, 2 * hidden), lambda e, info: (e, 0, 0))]
            + [WHOLE] * 3,
        ),
        compiler_params=limits(24),
        cost_estimate=cost(3e9, 1e7),
        name="first_quarter",
    )(info, xm, xt, mm, mt, w_gate, w_up)


def rest_kernel(parts, info, *refs):
    xs, (sel, back, weight, start, wg, wu, out, acc) = refs[: 2 * parts], refs[2 * parts :]
    step = pl.program_id(1)
    hidden, half = wg.shape[2], sel.shape[2]
    for j in range(parts):

        @pl.when(step == j)
        def _():
            rows = dot(sel[0], xs[2 * j][...]) + dot(sel[1], xs[2 * j + 1][...])
            rows = rows.astype(BF16)
            before = start[0] if j == 0 else acc[...]
            gate = before[:, :hidden] + dot(rows, wg[0])
            upper = before[:, hidden:] + dot(rows, wu[0])
            if j < parts - 1:
                acc[:, :hidden] = gate
                acc[:, hidden:] = upper
            else:
                act = gate / (1.0 + jnp.exp(-gate)) * upper * weight[:, 0:1]
                act = act.astype(BF16)
                count = act.shape[0]
                out[:half] = dot(back[0, 0, :, :count], act).astype(BF16)
                out[half:] = dot(back[1, 0, :, :count], act).astype(BF16)


def rest_quarters(order, xs, sel, back, weight, start, w_gate, w_up):
    local, hidden, width = w_gate.shape[0], w_gate.shape[2], xs[0].shape[1]
    parts = len(xs) // 2
    per_block, half = weight.shape[0] // local, sel.shape[2]
    weights = pl.BlockSpec((1, width, hidden), lambda e, j, order: (e, order[j], 0))
    return pl.pallas_call(
        functools.partial(rest_kernel, parts),
        out_shape=jax.ShapeDtypeStruct((2 * half, local * hidden), BF16),
        grid_spec=pltpu.PrefetchScalarGridSpec(
            num_scalar_prefetch=1,
            grid=(local, parts),
            in_specs=[WHOLE] * (2 * parts)
            + [
                pl.BlockSpec((2, per_block, half), lambda e, j, order: (0, e, 0)),
                pl.BlockSpec((2, 1, half, META), lambda e, j, order: (0, e, 0, 0)),
                pl.BlockSpec((per_block, META), lambda e, j, order: (e, 0)),
                pl.BlockSpec((1, per_block, 2 * hidden), lambda e, j, order: (e, 0, 0)),
                weights,
                weights,
            ],
            out_specs=pl.BlockSpec((2 * half, hidden), lambda e, j, order: (0, e)),
            scratch_shapes=[pltpu.VMEM((per_block, 2 * hidden), F32)],
        ),
        compiler_params=limits(32),
        cost_estimate=cost(9e9, 3e7),
        name="rest_quarters",
    )(order, *xs, sel, back, weight, start, w_gate, w_up)


def down_kernel(quarter, hid, wd, mine, twin, acc):
    step = pl.program_id(0)
    product = dot(hid[...], wd[0])
    half = mine.shape[0]

    @pl.when(step == 0)
    def _():
        acc[...] = product

    @pl.when(step > 0)
    def _():
        acc[...] += product

    @pl.when(step == pl.num_programs(0) - 1)
    def _():
        mine[...] = acc[:half]
        twin[...] = acc[half:].astype(BF16)


def down_quarter(quarter, hid, w_down, width):
    local, depth = w_down.shape[0], w_down.shape[1]
    half = hid.shape[0] // 2
    return pl.pallas_call(
        down_kernel,
        out_shape=[
            jax.ShapeDtypeStruct((half, width), F32),
            jax.ShapeDtypeStruct((half, width), BF16),
        ],
        grid_spec=pltpu.PrefetchScalarGridSpec(
            num_scalar_prefetch=1,
            grid=(local,),
            in_specs=[
                pl.BlockSpec((2 * half, depth), lambda e, q: (0, e)),
                pl.BlockSpec((1, depth, width), lambda e, q: (e, 0, q[0])),
            ],
            out_specs=[WHOLE] * 2,
            scratch_shapes=[pltpu.VMEM((2 * half, width), F32)],
        ),
        compiler_params=limits(24),
        cost_estimate=cost(1.8e9, 6e6),
        name="down_quarter",
    )(quarter, hid, w_down)


def join_kernel(chips, slots, own, twin, *refs):
    peers, outs = refs[: len(refs) - chips], refs[len(refs) - chips :]
    for k in range(chips):
        rows = pl.ds(k * slots, slots)
        total = own[rows, :] + twin[rows, :].astype(F32)
        for peer in peers:
            total += peer[rows, :].astype(F32)
        outs[k][...] = total.astype(BF16)


def join_partials(own, twin, peers, chips, slots):
    return pl.pallas_call(
        functools.partial(join_kernel, chips, slots),
        out_shape=[jax.ShapeDtypeStruct((slots, own.shape[1]), BF16)] * chips,
        in_specs=[WHOLE] * (2 + len(peers)),
        out_specs=[WHOLE] * chips,
        compiler_params=limits(16),
        cost_estimate=cost(5e8, 3e6),
        name="join_partials",
    )(own, twin, *peers)


def place_kernel(pick, *refs):
    blocks, out, held = refs[:-2], refs[-2], refs[-1]
    slots = blocks[0].shape[0]
    for k, block in enumerate(blocks):
        held[k * slots : (k + 1) * slots, :] = block[...]
    out[...] = dot(pick[...], held[...]).astype(BF16)


def place_rows(pick, blocks):
    width = blocks[0].shape[1]
    return pl.pallas_call(
        place_kernel,
        out_shape=jax.ShapeDtypeStruct((pick.shape[0], width), BF16),
        in_specs=[WHOLE] * (1 + len(blocks)),
        out_specs=WHOLE,
        scratch_shapes=[pltpu.VMEM((pick.shape[1], width), BF16)],
        compiler_params=limits(16),
        cost_estimate=cost(5e8, 1e6),
        name="place_rows",
    )(pick, *blocks)


def head_masks(heads, shape):
    lanes = iota(shape, 1)
    edge = heads * NOPE
    masks = []
    for h in range(heads):
        nope = (lanes >= h * NOPE) & (lanes < (h + 1) * NOPE)
        turned = (lanes >= edge + h * ROPE) & (lanes < edge + (h + 1) * ROPE)
        masks.append(nope | turned)
    return masks


def attend_prep_kernel(
    heads, latent, rope, lat_gain, key_up, value_up, queries, cosine, sine,
    to_q, to_q_pair, to_k, to_k_pair, gains, after, kv, stacked,
):
    nope, turned = heads * NOPE, heads * ROPE
    rows = latent.shape[0]
    cos, sin = cosine[...], sine[...]
    masks = head_masks(heads, (rows, nope + turned))

    def finish(values, pair, inverse, row):
        low = values[:, :nope] * inverse[:, :nope] * gains[row : row + 1, :nope]
        high = values[:, nope:] * gains[row : row + 1, nope:] * cos
        high = (high + pair * gains[row + 1 : row + 2, nope:] * sin) * inverse[:, nope:]
        return low.astype(BF16), high.astype(BF16)

    def spread(values, extra):
        squares = values * values
        total = jnp.zeros(values.shape, F32)
        for mask in masks:
            own = mask if values.shape[1] == nope + turned else mask[:, :nope]
            mean = (jnp.sum(jnp.where(own, squares, 0.0), axis=-1, keepdims=True) + extra) / QKD
            total = jnp.where(mask, lax.rsqrt(mean + EPS), total) if own is mask else total
        return total

    raw = queries[...]
    values, pair = dot(raw, to_q[...]), dot(raw, to_q_pair[...])
    low, high = finish(values, pair, spread(values, 0.0), 0)
    for h in range(heads):
        mine = pl.ds(h * rows, rows)
        stacked[mine, :nope] = jnp.where(masks[h][:, :nope], low.astype(F32), 0.0).astype(BF16)
        stacked[mine, nope:] = jnp.where(masks[h][:, nope:], high.astype(F32), 0.0).astype(BF16)

    lat = latent[...].astype(F32)
    scale = lax.rsqrt(jnp.mean(lat * lat, axis=-1, keepdims=True) + EPS)
    normed = (lat * scale * lat_gain[...]).astype(BF16)
    key_nope = dot(normed, key_up[...]).astype(BF16).astype(F32)
    shared = rope[...]
    shared_f = shared.astype(F32)
    extra = jnp.sum(shared_f * shared_f, axis=-1, keepdims=True)
    turned_k, pair_k = dot(shared, to_k[...]), dot(shared, to_k_pair[...])
    squares = key_nope * key_nope
    inverse = jnp.zeros((rows, nope + turned), F32)
    for mask in masks:
        total = jnp.sum(jnp.where(mask[:, :nope], squares, 0.0), axis=-1, keepdims=True)
        inverse = jnp.where(mask, lax.rsqrt((total + extra) / QKD + EPS), inverse)
    low, high = finish(jnp.concatenate([key_nope, turned_k], axis=1), pair_k, inverse, 2)
    kv[:, :nope] = low
    kv[:, nope : nope + turned] = high
    kv[:, nope + turned :] = dot(normed, value_up[...]).astype(BF16)


def rope_maps(heads):
    half = ROPE // 2
    nope, turned = heads * NOPE, heads * ROPE
    to_q = np.zeros((heads * QKD, nope + turned), np.float32)
    to_q_pair = np.zeros((heads * QKD, turned), np.float32)
    to_k = np.zeros((ROPE, turned), np.float32)
    to_k_pair = np.zeros((ROPE, turned), np.float32)
    for h in range(heads):
        for i in range(NOPE):
            to_q[h * QKD + i, h * NOPE + i] = 1
        for i in range(ROPE):
            other, sign = (i + half, -1) if i < half else (i - half, 1)
            to_q[h * QKD + NOPE + i, nope + h * ROPE + i] = 1
            to_q_pair[h * QKD + NOPE + other, h * ROPE + i] = sign
            to_k[i, h * ROPE + i] = 1
            to_k_pair[other, h * ROPE + i] = sign
    return [jnp.asarray(m, BF16) for m in (to_q, to_q_pair, to_k, to_k_pair)]


def attend_prep(me, latent, rope, lat_gain, key_up, value_up, queries, query_gain, key_gain, after):
    rows, heads = latent.shape[0], key_up.shape[1] // NOPE
    nope, turned = heads * NOPE, heads * ROPE
    half = ROPE // 2
    position = (me * rows + jnp.arange(rows, dtype=jnp.int32)).astype(F32)
    inverse = THETA ** (-jnp.arange(half, dtype=F32) / half)
    angles = position[:, None] * jnp.tile(inverse, turned // half)[None]

    def gain_rows(gain):
        tail = gain[NOPE:]
        swapped = jnp.concatenate([tail[half:], tail[:half]])
        own = jnp.concatenate([jnp.tile(gain[:NOPE], heads), jnp.tile(tail, heads)])
        pair = jnp.concatenate([jnp.zeros((nope,), F32), jnp.tile(swapped, heads)])
        return [own, pair]

    gains = jnp.stack(gain_rows(query_gain) + gain_rows(key_gain))
    return pl.pallas_call(
        functools.partial(attend_prep_kernel, heads),
        out_shape=[
            jax.ShapeDtypeStruct((rows, nope + turned + heads * VDIM), BF16),
            jax.ShapeDtypeStruct((heads * rows, nope + turned), BF16),
        ],
        in_specs=[WHOLE] * 13 + [ANY],
        out_specs=[WHOLE] * 2,
        compiler_params=limits(16),
        cost_estimate=cost(2e9, 4e6),
        name="attend_prep",
    )(
        latent, rope, lat_gain[None], key_up, value_up, queries, jnp.cos(angles),
        jnp.sin(angles), *rope_maps(heads), gains, after,
    )


def attend_kernel(heads, chips, info, stacked, *refs):
    blocks, (after, out, held) = refs[: 2 * chips], refs[2 * chips :]
    rows = out.shape[0]
    width = heads * (NOPE + ROPE)
    core, chip = info[1], info[2]
    query = stacked[...]
    shape = (heads * rows, rows)
    place = iota((heads * rows, 1), 0)
    for h in range(1, heads):
        place = place - jnp.where(iota((heads * rows, 1), 0) >= h * rows, rows, 0)
    query_pos = place + (chip * 2 + core) * rows
    for b in range(2 * chips):
        back, side = b % chips, b // chips
        source = (chip - back) * 2 + (core if side == 0 else 1 - core)
        first = jnp.where(chip >= back, source * rows, 1 << 30)
        scores = dot_nt(query, blocks[b][:, :width]) * (QKD ** (-0.5))
        seen = iota(shape, 1) + first <= query_pos
        held[:, b * rows : (b + 1) * rows] = jnp.where(seen, scores, -1e30)
    scores = held[...]
    expo = jnp.exp(scores - jnp.max(scores, axis=-1, keepdims=True))
    total = jnp.sum(expo, axis=-1, keepdims=True)
    probs = expo.astype(BF16)
    result = jnp.zeros((heads * rows, heads * VDIM), F32)
    for b in range(2 * chips):
        result += dot(probs[:, b * rows : (b + 1) * rows], blocks[b][:, width:])
    result = result / total
    lanes = iota((rows, heads * VDIM), 1)
    final = jnp.zeros((rows, heads * VDIM), F32)
    for h in range(heads):
        own = (lanes >= h * VDIM) & (lanes < (h + 1) * VDIM)
        final = jnp.where(own, result[h * rows : (h + 1) * rows], final)
    out[...] = final.astype(BF16)


def attend(info, stacked, blocks, heads, after):
    rows, chips = blocks[0].shape[0], len(blocks) // 2
    return pl.pallas_call(
        functools.partial(attend_kernel, heads, chips),
        out_shape=jax.ShapeDtypeStruct((rows, heads * VDIM), BF16),
        in_specs=[SCALARS] + [WHOLE] * (1 + len(blocks)) + [ANY],
        out_specs=WHOLE,
        scratch_shapes=[pltpu.VMEM((heads * rows, len(blocks) * rows), F32)],
        compiler_params=limits(24),
        cost_estimate=cost(5e9, 4e6),
        name="attend",
    )(info, stacked, *blocks, after)


def project_kernel(info, gain, proj, *refs):
    parts, out = refs[:-1], refs[-1]
    depth = parts[0].shape[1]
    total = jnp.zeros(out.shape, F32)
    squares = jnp.zeros((out.shape[0], 1), F32)
    for j, part in enumerate(parts):
        rows = pl.ds(pl.multiple_of((info[0] ^ j) * depth, 128), depth)
        value = part[...].astype(F32)
        squares += jnp.sum(value * value, axis=-1, keepdims=True)
        total += dot((value * gain[:, rows]).astype(BF16), proj[rows, :])
    out[...] = (total * lax.rsqrt(squares / (depth * len(parts)) + EPS)).astype(BF16)


def project(info, gain, proj, parts):
    return pl.pallas_call(
        project_kernel,
        out_shape=jax.ShapeDtypeStruct((parts[0].shape[0], proj.shape[1]), BF16),
        in_specs=[SCALARS] + [WHOLE] * (2 + len(parts)),
        out_specs=WHOLE,
        compiler_params=limits(16),
        cost_estimate=cost(1e9, 3e6),
        name="project",
    )(info, gain[None], proj, *parts)


def twin_shards(
    queries, kv_latent, rope_key, latent_gain, key_up, value_up, query_gain, key_gain, out_gain,
    out_proj, moe_input, moe_gain, expert_ids, route_weights, w_gate, w_up, w_down,
):
    ep, tp = lax.axis_size("ep"), lax.axis_size("tp")
    me, col = lax.axis_index("ep"), lax.axis_index("tp")
    chips, experts = ep // 2, ep * w_gate.shape[0]
    slots = PER_GROUP * CAP // TOP
    width = moe_input.shape[1] // tp
    heads = key_up.shape[1] // NOPE
    info = jnp.stack([col, me % 2, me // 2]).astype(jnp.int32)

    def along(values, step):
        return lax.ppermute(values, "ep", [(i, (i + 2 * step) % ep) for i in range(ep)])

    def later(values, step):
        return lax.ppermute(values, "ep", [(i, i + 2 * step) for i in range(ep - 2 * step)])

    def across(values):
        return lax.ppermute(values, "ep", [(i, i ^ 1) for i in range(ep)])

    def sideways(values, which):
        return lax.ppermute(values, "tp", [(i, i ^ which) for i in range(tp)])

    sources, diagonals, pick = make_dispatch(
        info, moe_input, moe_gain, expert_ids, route_weights, chips, experts, slots, width
    )
    arrived = [sources[0]] + [along(sources[k], k) for k in range(1, chips)]
    arrived_diag = [diagonals[0]] + [along(diagonals[k], k) for k in range(1, chips)]
    kv, stacked = attend_prep(
        me, kv_latent, rope_key, latent_gain, key_up, value_up, queries, query_gain, key_gain, pick
    )
    own = jnp.concatenate([block[:, :width] for block in arrived])
    meta = jnp.concatenate([block[:, width:] for block in arrived])
    own_twin, meta_twin = across(own), across(meta)
    beside = [sideways(own, 1), sideways(own, 2)]
    kv_blocks = [kv] + [later(kv, k) for k in range(1, chips)]
    kv_blocks = kv_blocks + [across(block) for block in kv_blocks]
    start, sel, back, weight = first_quarter(
        info, own, own_twin, meta, meta_twin, w_gate, w_up, chips, slots
    )
    beside.append(jnp.concatenate(arrived_diag))
    xs = []
    for block in beside:
        xs += [block, across(block)]
    order = jnp.stack([col ^ 1, col ^ 2, col ^ 3]).astype(jnp.int32)
    hidden = rest_quarters(order, xs, sel, back, weight, start, w_gate, w_up)
    peers = []
    for which in (3, 1, 2, 0):
        quarter = (col ^ which).astype(jnp.int32).reshape(1)
        mine, twin = down_quarter(quarter, hidden, w_down, width)
        twin = across(twin)
        if which:
            peers.append(sideways((mine + twin.astype(F32)).astype(BF16), which))
    attn = attend(info, stacked, kv_blocks, heads, mine)
    finished = join_partials(mine, twin, peers, chips, slots)
    returned = [finished[0]] + [along(finished[k], -k) for k in range(1, chips)]
    expert_out = place_rows(pick, returned)
    parts = [attn] + [sideways(attn, which) for which in range(1, tp)]
    mixed = project(info, out_gain, out_proj, parts)
    return (mixed, expert_out)


def fits_twins(mesh, w_gate):
    ep, tp = mesh.shape["ep"], mesh.shape["tp"]
    local = w_gate.shape[0] // ep
    return tp == 4 and ep % 2 == 0 and 2 * local == PER_GROUP and w_gate.shape[0] + ep // 2 <= META


def solution(mesh):
    in_specs = (
        P("ep", "tp"),
        P("ep", None),
        P("ep", None),
        P(),
        P(None, "tp"),
        P(None, "tp"),
        P(),
        P(),
        P(),
        P(None, "tp"),
        P("ep", None),
        P(),
        P("ep", None),
        P("ep", None),
        P("ep", None, "tp"),
        P("ep", None, "tp"),
        P("ep", "tp", None),
    )
    out_specs = (P("ep", "tp"), P("ep", "tp"))

    def step(*arrays):
        body = twin_shards if fits_twins(mesh, arrays[14]) else shards
        return jax.shard_map(
            body, mesh=mesh, in_specs=in_specs, out_specs=out_specs, check_vma=False
        )(*arrays)

    return step
```

```python
import functools

import jax
import jax.numpy as jnp
import numpy as np
from jax import lax
from jax.experimental import pallas as pl
from jax.experimental.pallas import tpu as pltpu
from jax.sharding import PartitionSpec as P

NOPE = 64
ROPE = 32
VDIM = 64
QKD = 96
CAP = 12
TOP = 2
PER_GROUP = 8


EPS = 1e-06
THETA = 10000.0


def rotate_half(values_in, positions):
    half_width = ROPE // 2
    inverse = THETA ** (-jnp.arange(half_width, dtype=jnp.float32) / half_width)
    angles = positions.astype(jnp.float32)[:, None] * inverse
    cosine = jnp.cos(angles)[:, None, :]
    sine = jnp.sin(angles)[:, None, :]
    first_half = values_in[..., :half_width]
    second_half = values_in[..., half_width:]
    return jnp.concatenate(
        [first_half * cosine - second_half * sine, second_half * cosine + first_half * sine],
        axis=-1,
    )


def head_norm(values_in, gain_vec):
    return (
        values_in
        * lax.rsqrt(jnp.mean(values_in * values_in, axis=-1, keepdims=True) + EPS)
        * gain_vec
    )


def make_queries(queries, query_gain, positions):
    row_count = queries.shape[0]
    head_count = queries.shape[1] // QKD
    normed = head_norm(queries.astype(jnp.float32).reshape(row_count, head_count, QKD), query_gain)
    turned = jnp.concatenate(
        [normed[..., :NOPE], rotate_half(normed[..., NOPE:], positions)], axis=-1
    )
    return turned.astype(jnp.bfloat16)


def make_keys(latent, rope_part, latent_gain, key_up, value_up, key_gain, positions):
    row_count = latent.shape[0]
    head_count = key_up.shape[1] // NOPE
    latent_f = latent.astype(jnp.float32)
    latent_n = (
        latent_f
        * lax.rsqrt(jnp.mean(latent_f * latent_f, axis=-1, keepdims=True) + EPS)
        * latent_gain
    ).astype(jnp.bfloat16)
    key_nope = jnp.dot(latent_n, key_up, preferred_element_type=jnp.float32).astype(jnp.bfloat16)
    key_nope = lax.optimization_barrier(key_nope)
    value_rows = jnp.dot(latent_n, value_up, preferred_element_type=jnp.float32).astype(
        jnp.bfloat16
    )
    shared = jnp.broadcast_to(
        rope_part.astype(jnp.float32)[:, None, :], (row_count, head_count, ROPE)
    )
    key_full = jnp.concatenate(
        [key_nope.astype(jnp.float32).reshape(row_count, head_count, NOPE), shared], axis=-1
    )
    normed = head_norm(key_full, key_gain)
    turned = jnp.concatenate(
        [normed[..., :NOPE], rotate_half(normed[..., NOPE:], positions)], axis=-1
    )
    return (turned.astype(jnp.bfloat16), value_rows.reshape(row_count, head_count, VDIM))


def shards(
    queries,
    kv_latent,
    rope_key,
    latent_gain,
    key_up,
    value_up,
    query_gain,
    key_gain,
    out_gain,
    out_proj,
    moe_input,
    moe_gain,
    expert_ids,
    route_weights,
    w_gate,
    w_up,
    w_down,
):
    tok_rows = queries.shape[0]
    head_count = key_up.shape[1] // NOPE
    query_pos = lax.axis_index("ep") * tok_rows + jnp.arange(tok_rows, dtype=jnp.int32)
    query_rot = make_queries(queries, query_gain, query_pos)
    inv_scale = QKD ** (-0.5)
    blocks_in = (
        lax.all_gather(kv_latent, "ep", axis=0, tiled=True),
        lax.all_gather(rope_key, "ep", axis=0, tiled=True),
    )
    key_pos = jnp.arange(blocks_in[0].shape[0], dtype=jnp.int32)
    key_rot, value_rows = make_keys(
        blocks_in[0], blocks_in[1], latent_gain, key_up, value_up, key_gain, key_pos
    )
    top_prev = jnp.full((head_count, tok_rows), -1e30, jnp.float32)
    key_pos = jnp.arange(key_rot.shape[0], dtype=jnp.int32)
    scores = (
        jnp.einsum("qhd,khd->hqk", query_rot, key_rot, preferred_element_type=jnp.float32)
        * inv_scale
    )
    visible = key_pos[None, :] <= query_pos[:, None]
    scores = jnp.where(visible[None], scores, -1e30)
    top_new = jnp.maximum(top_prev, jnp.max(scores, axis=-1))
    expo = jnp.exp(scores - top_new[..., None])
    total_new = jnp.sum(expo, axis=-1)
    accum_new = jnp.einsum(
        "hqk,khd->hqd", expo.astype(jnp.bfloat16), value_rows, preferred_element_type=jnp.float32
    )
    attn = (accum_new / total_new[..., None]).astype(jnp.bfloat16)
    attn = attn.transpose(1, 0, 2).reshape(tok_rows, head_count * VDIM)
    block_f = lax.all_gather(attn, "tp", axis=1, tiled=True).astype(jnp.float32)
    scaled = (block_f * out_gain[None, :]).astype(jnp.bfloat16)
    product = jnp.dot(scaled, out_proj, preferred_element_type=jnp.float32)
    product, squares = (product, jnp.sum(block_f * block_f, axis=-1))
    mixed = (product * lax.rsqrt(squares / out_gain.shape[0] + EPS)[:, None]).astype(jnp.bfloat16)
    row_count = moe_input.shape[0]
    top_count = expert_ids.shape[1]
    local_experts = w_gate.shape[0]
    ep_count = lax.axis_size("ep")
    expert_count = local_experts * ep_count
    stream_f = moe_input.astype(jnp.float32)
    normed = (
        stream_f * lax.rsqrt(jnp.mean(stream_f * stream_f, axis=-1, keepdims=True) + EPS) * moe_gain
    ).astype(jnp.bfloat16)
    flat_ids = expert_ids.reshape(-1)
    onehot = (flat_ids[:, None] == jnp.arange(expert_count, dtype=jnp.int32)[None, :]).astype(
        jnp.int32
    )
    slot_rank = jnp.sum((jnp.cumsum(onehot, axis=0) - onehot) * onehot, axis=1)
    slot_index = flat_ids * CAP + slot_rank
    token_index = jnp.arange(row_count * top_count, dtype=jnp.int32) // top_count
    slot_token = jnp.zeros((expert_count * CAP,), jnp.int32).at[slot_index].set(token_index)
    slot_used = jnp.zeros((expert_count * CAP,), jnp.bool_).at[slot_index].set(True)
    outgoing = jnp.where(slot_used[:, None], normed[slot_token], jnp.zeros((), jnp.bfloat16))
    outgoing = outgoing.reshape(ep_count, local_experts, CAP, normed.shape[1])
    piece_width = normed.shape[1] // lax.axis_size("tp")
    my_columns = lax.dynamic_slice_in_dim(
        outgoing, lax.axis_index("tp") * piece_width, piece_width, 3
    )
    arrived_part = lax.all_to_all(my_columns, "ep", split_axis=0, concat_axis=0, tiled=True)
    piece = lax.all_gather(arrived_part, "tp", axis=3, tiled=True)
    gate_acc = jnp.einsum("secd,edf->secf", piece, w_gate, preferred_element_type=jnp.float32)
    upper_acc = jnp.einsum("secd,edf->secf", piece, w_up, preferred_element_type=jnp.float32)
    hidden = (jax.nn.silu(gate_acc) * upper_acc).astype(jnp.bfloat16)
    out_cols = w_down.shape[2] // lax.axis_size("tp")
    term = jnp.einsum("secf,efd->dsec", hidden, w_down, preferred_element_type=jnp.float32)
    summed = lax.psum_scatter(
        term.reshape(lax.axis_size("tp") * out_cols, -1).astype(jnp.bfloat16),
        "tp",
        scatter_dimension=0,
        tiled=True,
    )
    expert_y = summed.T.reshape(ep_count, local_experts * CAP, out_cols)
    returned_rows = lax.all_to_all(expert_y, "ep", split_axis=0, concat_axis=0, tiled=True).reshape(
        expert_count * CAP, out_cols
    )
    picked = returned_rows[slot_index].reshape(row_count, top_count, out_cols).astype(jnp.float32)
    expert_out = jnp.sum(picked * route_weights[..., None], axis=1).astype(jnp.bfloat16)
    return (mixed, expert_out)


BF16 = jnp.bfloat16
F32 = jnp.float32
ANY = pl.BlockSpec(memory_space=pl.ANY)
WHOLE = pl.BlockSpec(memory_space=pltpu.VMEM)
META = 128


def iota(shape, dim):
    return lax.broadcasted_iota(jnp.int32, shape, dim)


def dot(left, right):
    return jnp.dot(left, right, preferred_element_type=F32)


def dot_nt(left, right):
    return lax.dot_general(left, right, (((1,), (1,)), ((), ())), preferred_element_type=F32)


def one_if(condition):
    return jnp.where(condition, 1.0, 0.0).astype(BF16)


def cost(flops, in_bytes):
    return pl.CostEstimate(flops=int(flops), bytes_accessed=int(in_bytes), transcendentals=0)


def limits(mib):
    return pltpu.CompilerParams(vmem_limit_bytes=mib * 1024 * 1024)


def in_hbm(values):
    return pltpu.with_memory_space_constraint(values, pltpu.HBM)


def start_all(pairs, sems):
    copies = [pltpu.make_async_copy(src, dst, sems.at[i]) for i, (src, dst) in enumerate(pairs)]
    for copy in copies:
        copy.start()
    return copies


def wait_all(copies):
    for copy in copies:
        copy.wait()


def dispatch_kernel(
    chips, experts, slots, x_hbm, gain_hbm, ids_hbm, route_hbm, *refs
):
    outs, (x_ref, gain_ref, ids_ref, route_ref, sems) = refs[:-5], refs[-5:]
    pairs = [(ids_hbm, ids_ref), (route_hbm, route_ref), (x_hbm, x_ref), (gain_hbm, gain_ref)]
    copies = start_all(pairs, sems)
    rows = x_ref.shape[0]
    width = outs[0].shape[1] - META
    sources, pick_ref = outs[:chips], outs[chips]
    chip = lax.shift_right_logical(lax.axis_index("ep"), 1)
    copies[0].wait()
    copies[1].wait()
    first, second = ids_ref[0:1, :], ids_ref[1:2, :]
    group = lax.shift_right_logical(first, jnp.int32(PER_GROUP.bit_length() - 1))
    target = group - chip
    target = jnp.where(target < 0, target + chips, target)
    places = iota((META, rows), 0)
    hot_first, hot_second = places == first, places == second
    hot_target = places == target + experts
    earlier = one_if(iota((rows, rows), 0) < iota((rows, rows), 1))
    counts = dot(one_if(hot_first | hot_second | hot_target), earlier)

    def at(mask):
        return jnp.sum(jnp.where(mask, counts, 0.0), axis=0, keepdims=True)

    slot = target.astype(F32) * slots + at(hot_target)
    values = [(first - group * PER_GROUP + 1).astype(F32), at(hot_first)]
    values += [(second - group * PER_GROUP + 1).astype(F32), at(hot_second)]
    for k in range(TOP):
        weight = route_ref[k : k + 1, :]
        high = weight.astype(BF16).astype(F32)
        middle = (weight - high).astype(BF16).astype(F32)
        values += [high, middle, weight - high - middle]
    meta = jnp.zeros((META, rows), F32)
    for place, value in enumerate(values):
        meta = jnp.where(places == place, value, meta)
    on_diagonal = iota((rows, rows), 0) == iota((rows, rows), 1)
    slot_col = jnp.sum(jnp.where(on_diagonal, slot, 0.0), axis=1, keepdims=True)
    pick_ref[...] = one_if(iota((rows, chips * slots), 1).astype(F32) == slot_col)
    select = one_if(iota((chips * slots, rows), 0).astype(F32) == slot)
    meta_rows = dot_nt(select, meta.astype(BF16)).astype(BF16)
    for k in range(chips):
        sources[k][:, width:] = meta_rows[k * slots : (k + 1) * slots]
    copies[2].wait()
    copies[3].wait()
    stream = x_ref[...].astype(F32)
    inverse = lax.rsqrt(jnp.mean(stream * stream, axis=-1, keepdims=True) + EPS)
    columns = pl.ds(pl.multiple_of(lax.axis_index("tp") * width, 128), width)
    part = x_ref[:, columns].astype(F32) * inverse * gain_ref[:, columns]
    picked = dot(select, part.astype(BF16)).astype(BF16)
    for k in range(chips):
        sources[k][:, :width] = picked[k * slots : (k + 1) * slots]


def scratch_like(*arrays):
    return [pltpu.VMEM(a.shape, a.dtype) for a in arrays] + [pltpu.SemaphoreType.DMA((len(arrays),))]


def make_dispatch(moe_input, moe_gain, expert_ids, route_weights, chips, experts, slots, width):
    rows = moe_input.shape[0]
    shapes = [jax.ShapeDtypeStruct((slots, width + META), BF16)] * chips
    shapes += [jax.ShapeDtypeStruct((rows, chips * slots), BF16)]
    arrays = (moe_input, moe_gain[None], expert_ids.T, route_weights.T)
    outs = pl.pallas_call(
        functools.partial(dispatch_kernel, chips, experts, slots),
        out_shape=shapes,
        in_specs=[ANY] * 4,
        out_specs=[WHOLE] * len(shapes),
        scratch_shapes=scratch_like(*arrays),
        compiler_params=limits(16),
        cost_estimate=cost(2e9, 4e6),
        name="dispatch",
    )(*[in_hbm(a) for a in arrays])
    return outs[:chips], outs[chips]


def stack_kernel(widths, count, *refs):
    blocks, outs = refs[:count], refs[count + 1 :]
    size = blocks[0].shape[0]
    for k, block in enumerate(blocks):
        first = 0
        for out, width in zip(outs, widths):
            out[k * size : (k + 1) * size, :] = block[:, first : first + width]
            first += width


def stack_blocks(blocks, widths, after):
    rows = len(blocks) * blocks[0].shape[0]
    return pl.pallas_call(
        functools.partial(stack_kernel, widths, len(blocks)),
        out_shape=[jax.ShapeDtypeStruct((rows, width), blocks[0].dtype) for width in widths],
        in_specs=[WHOLE] * len(blocks) + [ANY],
        out_specs=[WHOLE] * len(widths),
        compiler_params=limits(8),
        cost_estimate=cost(2e8, 1e6),
        name="stack_blocks",
    )(*blocks, after)


def up_pairs(wg, wu, out, which, first=0):
    count, width, hidden = out.shape[0], out.shape[1], wg.shape[2]
    rows = pl.ds(pl.multiple_of((lax.axis_index("tp") ^ which) * width, 128), width)
    pairs = []
    for e in range(count):
        pairs.append((wg.at[first + e, rows, :], out.at[e, :, pl.ds(0, hidden)]))
        pairs.append((wu.at[first + e, rows, :], out.at[e, :, pl.ds(hidden, hidden)]))
    return pairs


def down_pairs(wd, out, which):
    local, depth, width = wd.shape[0], wd.shape[1], out.shape[1]
    columns = pl.ds(pl.multiple_of((lax.axis_index("tp") ^ which) * width, 128), width)
    return [(wd.at[e, :, columns], out.at[pl.ds(e * depth, depth), :]) for e in range(local)]


def hold_up_kernel(wg, wu, after, near_x, near_y, sems):
    pairs = up_pairs(wg, wu, near_x, 1) + up_pairs(wg, wu, near_y, 2)
    wait_all(start_all(pairs, sems))


def hold_up(w_gate, w_up, width, after):
    local, columns = w_gate.shape[0], 2 * w_gate.shape[2]
    return pl.pallas_call(
        hold_up_kernel,
        out_shape=[
            jax.ShapeDtypeStruct((local, width, columns), BF16),
            jax.ShapeDtypeStruct((local // 2, width, columns), BF16),
        ],
        in_specs=[ANY] * 3,
        out_specs=[WHOLE] * 2,
        scratch_shapes=[pltpu.SemaphoreType.DMA((3 * local,))],
        compiler_params=limits(2),
        cost_estimate=cost(5e9, 3.4e7),
        name="hold_up",
    )(in_hbm(w_gate), in_hbm(w_up), after)


def first_kernel(
    chips, slots, local, xm, xt, mm, mt, wg, wu, acc, sel, back, weight, near_y, buf,
    own_sems, sems,
):
    pairs = up_pairs(wg, wu, buf, 0)
    start_all(pairs, own_sems)
    others = start_all(up_pairs(wg, wu, near_y, 2, local - near_y.shape[0]), sems)
    per_block, half = 2 * chips * CAP, chips * slots
    core = (lax.axis_index("ep") & 1).astype(F32)
    unit = one_if(iota((16, META), 0) == iota((16, META), 1))
    total = jnp.zeros((local * per_block, 1), F32)
    for side, meta_ref in ((0, mm), (1, mt)):
        meta = meta_ref[...]
        turned = dot_nt(unit, meta)
        cols = meta.astype(F32)

        def slot_of(take, block, k):
            expert = take(2 * k) - 1.0 - core * local
            inside = (expert >= 0.0) & (expert < local)
            return jnp.where(inside, expert * per_block + block * CAP + take(2 * k + 1), -1.0)

        def block_of(shape, dim):
            place = iota(shape, dim)
            block = jnp.full(shape, side * chips, jnp.int32)
            for k in range(1, chips):
                block = block + jnp.where(place >= k * slots, 1, 0)
            return block.astype(F32)

        def row_value(k):
            return turned[k : k + 1, :]

        def col_value(k):
            return cols[:, k : k + 1]

        places = iota((local * per_block, half), 0).astype(F32)
        hits = [places == slot_of(row_value, block_of((1, half), 1), k) for k in range(TOP)]
        for k in range(TOP):
            base = 2 * TOP + 3 * k
            share = row_value(base) + row_value(base + 1) + row_value(base + 2)
            total += jnp.sum(jnp.where(hits[k], share, 0.0), axis=-1, keepdims=True)
        sel[side] = one_if(hits[0] | hits[1])
        wanted = [slot_of(col_value, block_of((half, 1), 0), k) for k in range(TOP)]
        lanes = iota((half, local * per_block), 1).astype(F32)
        back[side] = one_if((lanes == wanted[0]) | (lanes == wanted[1]))
    weight[...] = jnp.broadcast_to(total, weight.shape)

    @pl.loop(0, local)
    def _(e):
        picked = picked_rows(sel, e, per_block, xm, xt)
        for j in range(2):
            pltpu.make_async_copy(*pairs[j], own_sems.at[2 * e + j]).wait()
        acc[e] = dot(picked, buf[e])

    wait_all(others)


def picked_rows(sel, e, count, mine, twin):
    own = pl.ds(pl.multiple_of(e * count, 16), count)
    return (dot(sel[0, own, :], mine[...]) + dot(sel[1, own, :], twin[...])).astype(BF16)


def first_quarter(xm, xt, mm, mt, w_gate, w_up, chips, slots):
    local, hidden, width = w_gate.shape[0], w_gate.shape[2], xm.shape[1]
    per_block, half = 2 * chips * CAP, chips * slots
    shapes = [
        jax.ShapeDtypeStruct((local, per_block, 2 * hidden), F32),
        jax.ShapeDtypeStruct((2, local * per_block, half), BF16),
        jax.ShapeDtypeStruct((2, half, local * per_block), BF16),
        jax.ShapeDtypeStruct((local * per_block, META), F32),
        jax.ShapeDtypeStruct((local - local // 2, width, 2 * hidden), BF16),
    ]
    return pl.pallas_call(
        functools.partial(first_kernel, chips, slots, local),
        out_shape=shapes,
        in_specs=[WHOLE] * 4 + [ANY] * 2,
        out_specs=[WHOLE] * 5,
        scratch_shapes=[
            pltpu.VMEM((local, width, 2 * hidden), BF16),
            pltpu.SemaphoreType.DMA((2 * local,)),
            pltpu.SemaphoreType.DMA((2 * (local - local // 2),)),
        ],
        compiler_params=limits(12),
        cost_estimate=cost(3e9, 1e7),
        name="first_quarter",
    )(xm, xt, mm, mt, in_hbm(w_gate), in_hbm(w_up))


def beside_kernel(xm, xt, ym, yt, sel, start, near_x, low_y, high_y, wg, wu, wd, acc, far, down, *sems):
    copies = start_all(up_pairs(wg, wu, far, 3), sems[0])
    copies += start_all(down_pairs(wd, down, 3), sems[1])
    _, per_block = start.shape[:2]
    count = low_y.shape[0]

    @pl.loop(0, count)
    def _(i):
        for e, y_ref in ((i, low_y), (i + count, high_y)):
            both = start[e] + dot(picked_rows(sel, e, per_block, xm, xt), near_x[e])
            acc[e] = both + dot(picked_rows(sel, e, per_block, ym, yt), y_ref[i])

    wait_all(copies)


def beside_quarters(xm, xt, ym, yt, sel, start, near_x, low_y, high_y, w_gate, w_up, w_down):
    local, width = near_x.shape[:2]
    return pl.pallas_call(
        beside_kernel,
        out_shape=[
            jax.ShapeDtypeStruct(start.shape, F32),
            jax.ShapeDtypeStruct(near_x.shape, BF16),
            jax.ShapeDtypeStruct((local * w_down.shape[1], width), BF16),
        ],
        in_specs=[WHOLE] * 9 + [ANY] * 3,
        out_specs=[WHOLE] * 3,
        scratch_shapes=[
            pltpu.SemaphoreType.DMA((2 * local,)),
            pltpu.SemaphoreType.DMA((local,)),
        ],
        compiler_params=limits(4),
        cost_estimate=cost(3e9, 1e7),
        name="beside_quarters",
    )(
        xm, xt, ym, yt, sel, start, near_x, low_y, high_y, in_hbm(w_gate), in_hbm(w_up),
        in_hbm(w_down),
    )


def far_kernel(m0, m1, t0, t1, sel, weight, start, far, wd, out, down_x, down_y, xm, xt, *sems):
    copies = start_all(down_pairs(wd, down_x, 1), sems[0])
    copies += start_all(down_pairs(wd, down_y, 2), sems[1])
    local, hidden = start.shape[0], start.shape[2] // 2
    per_block, half = start.shape[1], sel.shape[2]
    for whole, parts in ((xm, (m0, m1)), (xt, (t0, t1))):
        whole[: half // 2, :] = parts[0][...]
        whole[half // 2 :, :] = parts[1][...]

    @pl.loop(0, local // 2)
    def _(i):
        for e in (2 * i, 2 * i + 1):
            mine = pl.ds(pl.multiple_of(e * per_block, 16), per_block)
            both = start[e] + dot(picked_rows(sel, e, per_block, xm, xt), far[e])
            gate = both[:, :hidden]
            act = gate / (1.0 + jnp.exp(-gate)) * both[:, hidden:] * weight[mine, 0:1]
            out[mine, :] = act.astype(BF16)

    wait_all(copies)


def far_quarter(m0, m1, t0, t1, sel, weight, start, far, w_down):
    local, hidden, width, half = start.shape[0], start.shape[2] // 2, m0.shape[1], sel.shape[2]
    down = jax.ShapeDtypeStruct((local * w_down.shape[1], width), BF16)
    return pl.pallas_call(
        far_kernel,
        out_shape=[jax.ShapeDtypeStruct((sel.shape[1], hidden), BF16), down, down],
        in_specs=[WHOLE] * 8 + [ANY],
        out_specs=[WHOLE] * 3,
        scratch_shapes=[pltpu.VMEM((half, width), BF16)] * 2
        + [pltpu.SemaphoreType.DMA((local,))] * 2,
        compiler_params=limits(6),
        cost_estimate=cost(3e9, 1e7),
        name="far_quarter",
    )(m0, m1, t0, t1, sel, weight, start, far, in_hbm(w_down))


def split_kernel(x_ref, y_ref, first, second):
    rows = first.shape[0]
    first[...] = x_ref[:rows, :]
    second[...] = y_ref[rows:, :]


def split_halves(x_block, y_block):
    half = jax.ShapeDtypeStruct((x_block.shape[0] // 2, x_block.shape[1]), BF16)
    return pl.pallas_call(
        split_kernel,
        out_shape=[half, half],
        in_specs=[WHOLE] * 2,
        out_specs=[WHOLE] * 2,
        compiler_params=limits(4),
        cost_estimate=cost(1e8, 1e6),
        name="split_halves",
    )(x_block, y_block)


def down_kernel(local, acts, back, wd, mine, twin, held):
    count, depth = acts.shape[0] // local, acts.shape[1]
    for e in range(local):
        rows = pl.ds(e * count, count)
        held[rows, :] = dot(acts[rows, :], wd[e * depth : (e + 1) * depth, :]).astype(BF16)
    twin[...] = dot(back[1], held[...]).astype(BF16)
    mine[...] = dot(back[0], held[...])


def down_quarter(acts, back, wd):
    half, width = back.shape[1], wd.shape[1]
    return pl.pallas_call(
        functools.partial(down_kernel, wd.shape[0] // acts.shape[1]),
        out_shape=[
            jax.ShapeDtypeStruct((half, width), F32),
            jax.ShapeDtypeStruct((half, width), BF16),
        ],
        in_specs=[WHOLE] * 3,
        out_specs=[WHOLE] * 2,
        scratch_shapes=[pltpu.VMEM((acts.shape[0], width), BF16)],
        compiler_params=limits(4),
        cost_estimate=cost(1.8e9, 6e6),
        name="down_quarter",
    )(acts, back, wd)


def sum_kernel(first, mine, twin, *refs):
    extras, out = refs[:-1], refs[-1]
    rows = pl.ds(first, out.shape[0])
    total = mine[rows, :] + twin[rows, :].astype(F32)
    for extra in extras:
        total += extra[...].astype(F32)
    out[...] = total.astype(BF16)


def sum_half(second, mine, twin, *extras):
    rows = mine.shape[0] // 2
    return pl.pallas_call(
        functools.partial(sum_kernel, rows * second),
        out_shape=jax.ShapeDtypeStruct((rows, mine.shape[1]), BF16),
        in_specs=[WHOLE] * (2 + len(extras)),
        out_specs=WHOLE,
        compiler_params=limits(4),
        cost_estimate=cost(2e8, 1e6),
        name="sum_half",
    )(mine, twin, *extras)


def join_kernel(first, slots, own, twin, x_part, y_part, *outs):
    for k, out in enumerate(outs):
        near = pl.ds(k * slots, slots)
        rows = pl.ds(first + k * slots, slots)
        total = own[rows, :] + twin[rows, :].astype(F32)
        out[...] = (total + x_part[near, :].astype(F32) + y_part[near, :].astype(F32)).astype(BF16)


def join_half(second, own, twin, x_part, y_part, slots):
    rows, width = x_part.shape
    return pl.pallas_call(
        functools.partial(join_kernel, second * rows, slots),
        out_shape=[jax.ShapeDtypeStruct((slots, width), BF16)] * (rows // slots),
        in_specs=[WHOLE] * 4,
        out_specs=[WHOLE] * (rows // slots),
        compiler_params=limits(4),
        cost_estimate=cost(3e8, 2e6),
        name="join_half",
    )(own, twin, x_part, y_part)


def place_kernel(pick, *refs):
    blocks, out, held = refs[:-2], refs[-2], refs[-1]
    slots = blocks[0].shape[0]
    for k, block in enumerate(blocks):
        held[k * slots : (k + 1) * slots, :] = block[...]
    out[...] = dot(pick[...], held[...]).astype(BF16)


def place_rows(pick, blocks):
    width = blocks[0].shape[1]
    return pl.pallas_call(
        place_kernel,
        out_shape=jax.ShapeDtypeStruct((pick.shape[0], width), BF16),
        in_specs=[WHOLE] * (1 + len(blocks)),
        out_specs=WHOLE,
        scratch_shapes=[pltpu.VMEM((pick.shape[1], width), BF16)],
        compiler_params=limits(16),
        cost_estimate=cost(5e8, 1e6),
        name="place_rows",
    )(pick, *blocks)


def head_masks(heads, shape):
    lanes = iota(shape, 1)
    edge = heads * NOPE
    masks = []
    for h in range(heads):
        nope = (lanes >= h * NOPE) & (lanes < (h + 1) * NOPE)
        turned = (lanes >= edge + h * ROPE) & (lanes < edge + (h + 1) * ROPE)
        masks.append(nope | turned)
    return masks


def attend_prep_kernel(heads, count, *refs):
    sources, (after, kv, stacked) = refs[:count], refs[count : count + 3]
    held, sems = refs[count + 3 : -1], refs[-1]
    for copy in start_all(list(zip(sources, held)), sems):
        copy.wait()
    latent, rope, lat_gain, key_up, value_up, queries, q_gain, k_gain, rates, q_map, k_map, g_map = held
    nope, turned = heads * NOPE, heads * ROPE
    rows = latent.shape[0]
    position = iota((rows, turned), 0) + lax.axis_index("ep") * rows
    angles = position.astype(F32) * rates[...]
    cos, sin = jnp.cos(angles), jnp.sin(angles)
    masks = head_masks(heads, (rows, nope + turned))
    place = iota((8, QKD), 0)
    split = jnp.zeros((8, QKD), F32)
    for i, gain in enumerate((q_gain, k_gain)):
        whole = gain[...]
        high = whole.astype(BF16).astype(F32)
        middle = (whole - high).astype(BF16).astype(F32)
        for j, piece in enumerate((high, middle, whole - high - middle)):
            split = jnp.where(place == 3 * i + j, piece, split)
    spread = dot(split.astype(BF16), g_map[...])
    gains = [spread[i : i + 1] + spread[i + 1 : i + 2] + spread[i + 2 : i + 3] for i in (0, 3)]

    def finish(values, pair, inverse, gain):
        low = values[:, :nope] * inverse[:, :nope] * gain[:, :nope]
        high = values[:, nope:] * gain[:, nope : nope + turned] * cos
        high = (high + pair * gain[:, nope + turned :] * sin) * inverse[:, nope:]
        return low, high

    both = dot(queries[...], q_map[...])
    values, pair = both[:, : nope + turned], both[:, nope + turned :]
    squares = values * values
    inverse = jnp.zeros(values.shape, F32)
    for mask in masks:
        total = jnp.sum(jnp.where(mask, squares, 0.0), axis=-1, keepdims=True)
        inverse = jnp.where(mask, lax.rsqrt(total / QKD + EPS), inverse)
    low, high = finish(values, pair, inverse, gains[0])
    for h in range(heads):
        mine = pl.ds(h * rows, rows)
        stacked[mine, :nope] = jnp.where(masks[h][:, :nope], low, 0.0).astype(BF16)
        stacked[mine, nope:] = jnp.where(masks[h][:, nope:], high, 0.0).astype(BF16)

    lat = latent[...].astype(F32)
    scale = lax.rsqrt(jnp.mean(lat * lat, axis=-1, keepdims=True) + EPS)
    normed = (lat * scale * lat_gain[...]).astype(BF16)
    key_nope = dot(normed, key_up[...]).astype(BF16).astype(F32)
    shared = lax.dot_general(
        rope[...], k_map[...], (((0,), (0,)), ((), ())), preferred_element_type=F32
    )
    turned_k, pair_k = shared[:, :turned], shared[:, turned:]
    values = jnp.concatenate([key_nope, turned_k], axis=1)
    squares = values * values
    inverse = jnp.zeros(values.shape, F32)
    for mask in masks:
        total = jnp.sum(jnp.where(mask, squares, 0.0), axis=-1, keepdims=True)
        inverse = jnp.where(mask, lax.rsqrt(total / QKD + EPS), inverse)
    low, high = finish(values, pair_k, inverse, gains[1])
    kv[:, :nope] = low.astype(BF16)
    kv[:, nope : nope + turned] = high.astype(BF16)
    kv[:, nope + turned :] = dot(normed, value_up[...]).astype(BF16)


def rope_maps(heads):
    half = ROPE // 2
    nope, turned = heads * NOPE, heads * ROPE
    q_map = np.zeros((heads * QKD, nope + 2 * turned), np.float32)
    k_map = np.zeros((ROPE, 2 * turned), np.float32)
    g_map = np.zeros((QKD, nope + 2 * turned), np.float32)
    for h in range(heads):
        for i in range(NOPE):
            q_map[h * QKD + i, h * NOPE + i] = 1
        for i in range(ROPE):
            other, sign = (i + half, -1) if i < half else (i - half, 1)
            at = h * ROPE + i
            q_map[h * QKD + NOPE + i, nope + at] = 1
            q_map[h * QKD + NOPE + other, nope + turned + at] = sign
            k_map[i, at] = 1
            k_map[other, turned + at] = sign
        g_map += np.abs(q_map[h * QKD : (h + 1) * QKD])
    rates = np.tile(np.float32(THETA) ** (-np.arange(half, dtype=np.float32) / half), turned // half)
    return [jnp.asarray(rates[None], F32)] + [jnp.asarray(m, BF16) for m in (q_map, k_map, g_map)]


def attend_prep(latent, rope, lat_gain, key_up, value_up, queries, query_gain, key_gain, after):
    rows, heads = latent.shape[0], key_up.shape[1] // NOPE
    wide = heads * (NOPE + ROPE)
    arrays = [latent, rope.T, lat_gain[None], key_up, value_up, queries]
    arrays += [query_gain[None], key_gain[None]] + rope_maps(heads)
    return pl.pallas_call(
        functools.partial(attend_prep_kernel, heads, len(arrays)),
        out_shape=[
            jax.ShapeDtypeStruct((rows, wide + heads * VDIM), BF16),
            jax.ShapeDtypeStruct((heads * rows, wide), BF16),
        ],
        in_specs=[ANY] * (len(arrays) + 1),
        out_specs=[WHOLE] * 2,
        scratch_shapes=scratch_like(*arrays),
        compiler_params=limits(8),
        cost_estimate=cost(2e9, 4e6),
        name="attend_prep",
    )(*[in_hbm(a) for a in arrays], after)


def attend_kernel(heads, chips, stacked, mine, twin, wd, out, down, held, mixed, sems):
    copies = start_all(down_pairs(wd, down, 0), sems)
    rows = out.shape[0]
    width = heads * (NOPE + ROPE)
    core = lax.axis_index("ep") & 1
    chip = lax.shift_right_logical(lax.axis_index("ep"), 1)
    place = iota((heads * rows, 1), 0)
    for h in range(1, heads):
        place = place - jnp.where(iota((heads * rows, 1), 0) >= h * rows, rows, 0)
    query_pos = place + lax.axis_index("ep") * rows

    @pl.loop(0, chips)
    def _(back):
        where = pl.ds(pl.multiple_of(back * rows, 128), rows)
        for side, keys in ((0, mine), (1, twin)):
            source = (chip - back) * 2 + (core if side == 0 else 1 - core)
            first = jnp.where(chip >= back, source * rows, 1 << 30)
            scores = dot_nt(stacked[...], keys[where, :width]) * (QKD ** (-0.5))
            seen = iota((heads * rows, rows), 1) + first <= query_pos
            lanes = pl.ds(pl.multiple_of((side * chips + back) * rows, 128), rows)
            held[:, lanes] = jnp.where(seen, scores, -1e30)

    mixed[...] = jnp.zeros(mixed.shape, F32)
    size = chips * rows
    lanes = iota((rows, heads * VDIM), 1)

    @pl.loop(0, heads // 2)
    def _(i):
        for h in (2 * i, 2 * i + 1):
            scores = held[pl.ds(pl.multiple_of(h * rows, 128), rows), :]
            expo = jnp.exp(scores - jnp.max(scores, axis=-1, keepdims=True))
            total = jnp.sum(expo, axis=-1, keepdims=True)
            probs = expo.astype(BF16)
            result = dot(probs[:, :size], mine[:, width:]) + dot(probs[:, size:], twin[:, width:])
            own = (lanes >= h * VDIM) & (lanes < (h + 1) * VDIM)
            mixed[...] += jnp.where(own, result / total, 0.0)

    out[...] = mixed[...].astype(BF16)
    wait_all(copies)


def attend(stacked, mine, twin, w_down, width, heads, chips):
    rows, local = stacked.shape[0] // heads, w_down.shape[0]
    return pl.pallas_call(
        functools.partial(attend_kernel, heads, chips),
        out_shape=[
            jax.ShapeDtypeStruct((rows, heads * VDIM), BF16),
            jax.ShapeDtypeStruct((local * w_down.shape[1], width), BF16),
        ],
        in_specs=[WHOLE] * 3 + [ANY],
        out_specs=[WHOLE] * 2,
        scratch_shapes=[
            pltpu.VMEM((heads * rows, 2 * chips * rows), F32),
            pltpu.VMEM((rows, heads * VDIM), F32),
            pltpu.SemaphoreType.DMA((local,)),
        ],
        compiler_params=limits(12),
        cost_estimate=cost(5e9, 4e6),
        name="attend",
    )(stacked, mine, twin, in_hbm(w_down))


def project_kernel(gain, proj, *refs):
    parts, out = refs[:-1], refs[-1]
    depth = parts[0].shape[1]
    total = jnp.zeros(out.shape, F32)
    squares = jnp.zeros((out.shape[0], 1), F32)
    for j, part in enumerate(parts):
        rows = pl.ds(pl.multiple_of((lax.axis_index("tp") ^ j) * depth, 128), depth)
        value = part[...].astype(F32)
        squares += jnp.sum(value * value, axis=-1, keepdims=True)
        total += dot((value * gain[:, rows]).astype(BF16), proj[rows, :])
    out[...] = (total * lax.rsqrt(squares / (depth * len(parts)) + EPS)).astype(BF16)


def project(gain, proj, parts):
    return pl.pallas_call(
        project_kernel,
        out_shape=jax.ShapeDtypeStruct((parts[0].shape[0], proj.shape[1]), BF16),
        in_specs=[WHOLE] * (2 + len(parts)),
        out_specs=WHOLE,
        compiler_params=limits(16),
        cost_estimate=cost(1e9, 3e6),
        name="project",
    )(gain[None], proj, *parts)


def twin_shards(
    queries, kv_latent, rope_key, latent_gain, key_up, value_up, query_gain, key_gain, out_gain,
    out_proj, moe_input, moe_gain, expert_ids, route_weights, w_gate, w_up, w_down,
):
    ep, tp = lax.axis_size("ep"), lax.axis_size("tp")
    chips, experts = ep // 2, ep * w_gate.shape[0]
    slots = PER_GROUP * CAP // TOP
    width = moe_input.shape[1] // tp
    heads = key_up.shape[1] // NOPE

    def send(values, axis, pairs):
        return lax.ppermute(values, axis, pairs)

    def along(values, shift):
        return send(values, "ep", [(i, (i + 2 * shift) % ep) for i in range(ep)])

    def across(values):
        return send(values, "ep", [(i, i ^ 1) for i in range(ep)])

    def sideways(values, which):
        return send(values, "tp", [(i, i ^ which) for i in range(tp)])

    others, middle = range(1, chips), chips // 2
    sources, pick = make_dispatch(
        moe_input, moe_gain, expert_ids, route_weights, chips, experts, slots, width
    )
    arrived = [sources[0]] + [along(sources[k], k) for k in others]
    near_x, low_y = hold_up(w_gate, w_up, width, pick)
    kv, stacked = attend_prep(
        kv_latent, rope_key, latent_gain, key_up, value_up, queries, query_gain,
        key_gain, pick,
    )
    own, meta = stack_blocks(arrived, (width, META), near_x)
    own_twin, meta_twin = across(own), across(meta)
    x_block, y_block = sideways(own, 1), sideways(own, 2)
    kv_blocks = [kv] + [along(kv, k) for k in others]
    start, sel, back, weight, high_y = first_quarter(
        own, own_twin, meta, meta_twin, w_gate, w_up, chips, slots
    )
    x_half, y_half = split_halves(x_block, y_block)
    far_first, far_second = sideways(x_half, 2), sideways(y_half, 1)
    x_twin, y_twin = across(x_block), across(y_block)
    start, far_weights, down_d = beside_quarters(
        x_block, x_twin, y_block, y_twin, sel, start, near_x, low_y, high_y,
        w_gate, w_up, w_down,
    )
    twin_first, twin_second = across(far_first), across(far_second)
    (kv_mine,) = stack_blocks(kv_blocks, (kv.shape[1],), kv)
    kv_twin = across(kv_mine)
    acts, down_x, down_y = far_quarter(
        far_first, far_second, twin_first, twin_second, sel, weight, start,
        far_weights, w_down,
    )
    d_mine, d_twin = down_quarter(acts, back, down_d)
    d_twin = across(d_twin)
    x_mine, x_twin = down_quarter(acts, back, down_x)
    x_twin = across(x_twin)
    from_y = sideways(sum_half(1, d_mine, d_twin), 2)
    from_x = sideways(sum_half(0, d_mine, d_twin), 1)
    y_mine, y_twin = down_quarter(acts, back, down_y)
    y_twin = across(y_twin)
    x_first = sideways(sum_half(0, x_mine, x_twin), 1)
    y_second = sideways(sum_half(1, y_mine, y_twin), 2)
    x_second = sideways(sum_half(1, x_mine, x_twin, from_y), 1)
    y_first = sideways(sum_half(0, y_mine, y_twin, from_x), 2)
    attn, down_own = attend(stacked, kv_mine, kv_twin, w_down, width, heads, chips)
    mine, twin = down_quarter(acts, back, down_own)
    twin = across(twin)
    parts = [attn] + [sideways(attn, which) for which in range(1, tp)]
    second = join_half(1, mine, twin, x_second, y_second, slots)
    returned = [along(block, -k) for k, block in enumerate(second, middle)]
    first = join_half(0, mine, twin, x_first, y_first, slots)
    returned = [along(first[k], -k) for k in range(1, middle)] + returned
    mixed = project(out_gain, out_proj, parts)
    expert_out = place_rows(pick, [first[0]] + returned)
    return (mixed, expert_out)


def fits_twins(mesh, w_gate):
    ep, tp = mesh.shape["ep"], mesh.shape["tp"]
    local = w_gate.shape[0] // ep
    return tp == 4 and ep % 4 == 0 and local % 2 == 0 and 2 * local == PER_GROUP and w_gate.shape[0] + ep // 2 <= META


def solution(mesh):
    in_specs = (
        P("ep", "tp"),
        P("ep", None),
        P("ep", None),
        P(),
        P(None, "tp"),
        P(None, "tp"),
        P(),
        P(),
        P(),
        P(None, "tp"),
        P("ep", None),
        P(),
        P("ep", None),
        P("ep", None),
        P("ep", None, "tp"),
        P("ep", None, "tp"),
        P("ep", "tp", None),
    )
    out_specs = (P("ep", "tp"), P("ep", "tp"))

    def mapped(body):
        return jax.shard_map(
            body, mesh=mesh, in_specs=in_specs, out_specs=out_specs, check_vma=False
        )

    def step(*arrays):
        if not fits_twins(mesh, arrays[14]):
            return mapped(shards)(*arrays)
        return mapped(twin_shards)(*arrays)

    return step
```

```python
import functools

import jax
import jax.numpy as jnp
import numpy as np
from jax import lax
from jax.experimental import pallas as pl
from jax.experimental.pallas import tpu as pltpu
from jax.sharding import PartitionSpec as P

NOPE = 64
ROPE = 32
VDIM = 64
QKD = 96
CAP = 12
TOP = 2
PER_GROUP = 8


EPS = 1e-06
THETA = 10000.0


def rotate_half(values_in, positions):
    half_width = ROPE // 2
    inverse = THETA ** (-jnp.arange(half_width, dtype=jnp.float32) / half_width)
    angles = positions.astype(jnp.float32)[:, None] * inverse
    cosine = jnp.cos(angles)[:, None, :]
    sine = jnp.sin(angles)[:, None, :]
    first_half = values_in[..., :half_width]
    second_half = values_in[..., half_width:]
    return jnp.concatenate(
        [first_half * cosine - second_half * sine, second_half * cosine + first_half * sine],
        axis=-1,
    )


def head_norm(values_in, gain_vec):
    return (
        values_in
        * lax.rsqrt(jnp.mean(values_in * values_in, axis=-1, keepdims=True) + EPS)
        * gain_vec
    )


def make_queries(queries, query_gain, positions):
    row_count = queries.shape[0]
    head_count = queries.shape[1] // QKD
    normed = head_norm(queries.astype(jnp.float32).reshape(row_count, head_count, QKD), query_gain)
    turned = jnp.concatenate(
        [normed[..., :NOPE], rotate_half(normed[..., NOPE:], positions)], axis=-1
    )
    return turned.astype(jnp.bfloat16)


def make_keys(latent, rope_part, latent_gain, key_up, value_up, key_gain, positions):
    row_count = latent.shape[0]
    head_count = key_up.shape[1] // NOPE
    latent_f = latent.astype(jnp.float32)
    latent_n = (
        latent_f
        * lax.rsqrt(jnp.mean(latent_f * latent_f, axis=-1, keepdims=True) + EPS)
        * latent_gain
    ).astype(jnp.bfloat16)
    key_nope = jnp.dot(latent_n, key_up, preferred_element_type=jnp.float32).astype(jnp.bfloat16)
    key_nope = lax.optimization_barrier(key_nope)
    value_rows = jnp.dot(latent_n, value_up, preferred_element_type=jnp.float32).astype(
        jnp.bfloat16
    )
    shared = jnp.broadcast_to(
        rope_part.astype(jnp.float32)[:, None, :], (row_count, head_count, ROPE)
    )
    key_full = jnp.concatenate(
        [key_nope.astype(jnp.float32).reshape(row_count, head_count, NOPE), shared], axis=-1
    )
    normed = head_norm(key_full, key_gain)
    turned = jnp.concatenate(
        [normed[..., :NOPE], rotate_half(normed[..., NOPE:], positions)], axis=-1
    )
    return (turned.astype(jnp.bfloat16), value_rows.reshape(row_count, head_count, VDIM))


def shards(
    queries,
    kv_latent,
    rope_key,
    latent_gain,
    key_up,
    value_up,
    query_gain,
    key_gain,
    out_gain,
    out_proj,
    moe_input,
    moe_gain,
    expert_ids,
    route_weights,
    w_gate,
    w_up,
    w_down,
):
    tok_rows = queries.shape[0]
    head_count = key_up.shape[1] // NOPE
    query_pos = lax.axis_index("ep") * tok_rows + jnp.arange(tok_rows, dtype=jnp.int32)
    query_rot = make_queries(queries, query_gain, query_pos)
    inv_scale = QKD ** (-0.5)
    blocks_in = (
        lax.all_gather(kv_latent, "ep", axis=0, tiled=True),
        lax.all_gather(rope_key, "ep", axis=0, tiled=True),
    )
    key_pos = jnp.arange(blocks_in[0].shape[0], dtype=jnp.int32)
    key_rot, value_rows = make_keys(
        blocks_in[0], blocks_in[1], latent_gain, key_up, value_up, key_gain, key_pos
    )
    top_prev = jnp.full((head_count, tok_rows), -1e30, jnp.float32)
    key_pos = jnp.arange(key_rot.shape[0], dtype=jnp.int32)
    scores = (
        jnp.einsum("qhd,khd->hqk", query_rot, key_rot, preferred_element_type=jnp.float32)
        * inv_scale
    )
    visible = key_pos[None, :] <= query_pos[:, None]
    scores = jnp.where(visible[None], scores, -1e30)
    top_new = jnp.maximum(top_prev, jnp.max(scores, axis=-1))
    expo = jnp.exp(scores - top_new[..., None])
    total_new = jnp.sum(expo, axis=-1)
    accum_new = jnp.einsum(
        "hqk,khd->hqd", expo.astype(jnp.bfloat16), value_rows, preferred_element_type=jnp.float32
    )
    attn = (accum_new / total_new[..., None]).astype(jnp.bfloat16)
    attn = attn.transpose(1, 0, 2).reshape(tok_rows, head_count * VDIM)
    block_f = lax.all_gather(attn, "tp", axis=1, tiled=True).astype(jnp.float32)
    scaled = (block_f * out_gain[None, :]).astype(jnp.bfloat16)
    product = jnp.dot(scaled, out_proj, preferred_element_type=jnp.float32)
    product, squares = (product, jnp.sum(block_f * block_f, axis=-1))
    mixed = (product * lax.rsqrt(squares / out_gain.shape[0] + EPS)[:, None]).astype(jnp.bfloat16)
    row_count = moe_input.shape[0]
    top_count = expert_ids.shape[1]
    local_experts = w_gate.shape[0]
    ep_count = lax.axis_size("ep")
    expert_count = local_experts * ep_count
    stream_f = moe_input.astype(jnp.float32)
    normed = (
        stream_f * lax.rsqrt(jnp.mean(stream_f * stream_f, axis=-1, keepdims=True) + EPS) * moe_gain
    ).astype(jnp.bfloat16)
    flat_ids = expert_ids.reshape(-1)
    onehot = (flat_ids[:, None] == jnp.arange(expert_count, dtype=jnp.int32)[None, :]).astype(
        jnp.int32
    )
    slot_rank = jnp.sum((jnp.cumsum(onehot, axis=0) - onehot) * onehot, axis=1)
    slot_index = flat_ids * CAP + slot_rank
    token_index = jnp.arange(row_count * top_count, dtype=jnp.int32) // top_count
    slot_token = jnp.zeros((expert_count * CAP,), jnp.int32).at[slot_index].set(token_index)
    slot_used = jnp.zeros((expert_count * CAP,), jnp.bool_).at[slot_index].set(True)
    outgoing = jnp.where(slot_used[:, None], normed[slot_token], jnp.zeros((), jnp.bfloat16))
    outgoing = outgoing.reshape(ep_count, local_experts, CAP, normed.shape[1])
    piece_width = normed.shape[1] // lax.axis_size("tp")
    my_columns = lax.dynamic_slice_in_dim(
        outgoing, lax.axis_index("tp") * piece_width, piece_width, 3
    )
    arrived_part = lax.all_to_all(my_columns, "ep", split_axis=0, concat_axis=0, tiled=True)
    piece = lax.all_gather(arrived_part, "tp", axis=3, tiled=True)
    gate_acc = jnp.einsum("secd,edf->secf", piece, w_gate, preferred_element_type=jnp.float32)
    upper_acc = jnp.einsum("secd,edf->secf", piece, w_up, preferred_element_type=jnp.float32)
    hidden = (jax.nn.silu(gate_acc) * upper_acc).astype(jnp.bfloat16)
    out_cols = w_down.shape[2] // lax.axis_size("tp")
    term = jnp.einsum("secf,efd->dsec", hidden, w_down, preferred_element_type=jnp.float32)
    summed = lax.psum_scatter(
        term.reshape(lax.axis_size("tp") * out_cols, -1).astype(jnp.bfloat16),
        "tp",
        scatter_dimension=0,
        tiled=True,
    )
    expert_y = summed.T.reshape(ep_count, local_experts * CAP, out_cols)
    returned_rows = lax.all_to_all(expert_y, "ep", split_axis=0, concat_axis=0, tiled=True).reshape(
        expert_count * CAP, out_cols
    )
    picked = returned_rows[slot_index].reshape(row_count, top_count, out_cols).astype(jnp.float32)
    expert_out = jnp.sum(picked * route_weights[..., None], axis=1).astype(jnp.bfloat16)
    return (mixed, expert_out)


BF16 = jnp.bfloat16
F32 = jnp.float32
ANY = pl.BlockSpec(memory_space=pl.ANY)
WHOLE = pl.BlockSpec(memory_space=pltpu.VMEM)
META = 128


def iota(shape, dim):
    return lax.broadcasted_iota(jnp.int32, shape, dim)


def dot(left, right):
    return jnp.dot(left, right, preferred_element_type=F32)


def dot_nt(left, right):
    return lax.dot_general(left, right, (((1,), (1,)), ((), ())), preferred_element_type=F32)


def one_if(condition):
    return jnp.where(condition, 1.0, 0.0).astype(BF16)


def cost(flops, in_bytes):
    return pl.CostEstimate(flops=int(flops), bytes_accessed=int(in_bytes), transcendentals=0)


def limits(mib):
    return pltpu.CompilerParams(vmem_limit_bytes=mib * 1024 * 1024)


def in_hbm(values):
    return pltpu.with_memory_space_constraint(values, pltpu.HBM)


def start_all(pairs, sems):
    copies = [pltpu.make_async_copy(src, dst, sems.at[i]) for i, (src, dst) in enumerate(pairs)]
    for copy in copies:
        copy.start()
    return copies


def wait_all(copies):
    for copy in copies:
        copy.wait()


def dispatch_kernel(
    chips, experts, slots, x_hbm, gain_hbm, ids_hbm, route_hbm, *refs
):
    outs, (x_ref, gain_ref, ids_ref, route_ref, sems) = refs[:-5], refs[-5:]
    pairs = [(ids_hbm, ids_ref), (route_hbm, route_ref), (x_hbm, x_ref), (gain_hbm, gain_ref)]
    copies = start_all(pairs, sems)
    rows = x_ref.shape[0]
    width = outs[0].shape[1] - META
    sources, pick_ref = outs[:chips], outs[chips]
    chip = lax.shift_right_logical(lax.axis_index("ep"), 1)
    copies[0].wait()
    copies[1].wait()
    first, second = ids_ref[0:1, :], ids_ref[1:2, :]
    group = lax.shift_right_logical(first, jnp.int32(PER_GROUP.bit_length() - 1))
    target = group - chip
    target = jnp.where(target < 0, target + chips, target)
    places = iota((META, rows), 0)
    hot_first, hot_second = places == first, places == second
    hot_target = places == target + experts
    earlier = one_if(iota((rows, rows), 0) < iota((rows, rows), 1))
    counts = dot(one_if(hot_first | hot_second | hot_target), earlier)

    def at(mask):
        return jnp.sum(jnp.where(mask, counts, 0.0), axis=0, keepdims=True)

    slot = target.astype(F32) * slots + at(hot_target)
    values = [(first - group * PER_GROUP + 1).astype(F32), at(hot_first)]
    values += [(second - group * PER_GROUP + 1).astype(F32), at(hot_second)]
    for k in range(TOP):
        weight = route_ref[k : k + 1, :]
        high = weight.astype(BF16).astype(F32)
        middle = (weight - high).astype(BF16).astype(F32)
        values += [high, middle, weight - high - middle]
    meta = jnp.zeros((META, rows), F32)
    for place, value in enumerate(values):
        meta = jnp.where(places == place, value, meta)
    on_diagonal = iota((rows, rows), 0) == iota((rows, rows), 1)
    slot_col = jnp.sum(jnp.where(on_diagonal, slot, 0.0), axis=1, keepdims=True)
    pick_ref[...] = one_if(iota((rows, chips * slots), 1).astype(F32) == slot_col)
    select = one_if(iota((chips * slots, rows), 0).astype(F32) == slot)
    meta_rows = dot_nt(select, meta.astype(BF16)).astype(BF16)
    for k in range(chips):
        sources[k][:, width:] = meta_rows[k * slots : (k + 1) * slots]
    copies[2].wait()
    copies[3].wait()
    stream = x_ref[...].astype(F32)
    inverse = lax.rsqrt(jnp.mean(stream * stream, axis=-1, keepdims=True) + EPS)
    columns = pl.ds(pl.multiple_of(lax.axis_index("tp") * width, 128), width)
    part = x_ref[:, columns].astype(F32) * inverse * gain_ref[:, columns]
    picked = dot(select, part.astype(BF16)).astype(BF16)
    for k in range(chips):
        sources[k][:, :width] = picked[k * slots : (k + 1) * slots]


def scratch_like(*arrays):
    return [pltpu.VMEM(a.shape, a.dtype) for a in arrays] + [pltpu.SemaphoreType.DMA((len(arrays),))]


def make_dispatch(moe_input, moe_gain, expert_ids, route_weights, chips, experts, slots, width):
    rows = moe_input.shape[0]
    shapes = [jax.ShapeDtypeStruct((slots, width + META), BF16)] * chips
    shapes += [jax.ShapeDtypeStruct((rows, chips * slots), BF16)]
    arrays = (moe_input, moe_gain[None], expert_ids.T, route_weights.T)
    outs = pl.pallas_call(
        functools.partial(dispatch_kernel, chips, experts, slots),
        out_shape=shapes,
        in_specs=[ANY] * 4,
        out_specs=[WHOLE] * len(shapes),
        scratch_shapes=scratch_like(*arrays),
        compiler_params=limits(16),
        cost_estimate=cost(2e9, 4e6),
        name="dispatch",
    )(*[in_hbm(a) for a in arrays])
    return outs[:chips], outs[chips]


def stack_kernel(widths, count, *refs):
    blocks, outs = refs[:count], refs[count + 1 :]
    size = blocks[0].shape[0]
    for k, block in enumerate(blocks):
        first = 0
        for out, width in zip(outs, widths):
            out[k * size : (k + 1) * size, :] = block[:, first : first + width]
            first += width


def stack_blocks(blocks, widths, after):
    rows = len(blocks) * blocks[0].shape[0]
    return pl.pallas_call(
        functools.partial(stack_kernel, widths, len(blocks)),
        out_shape=[jax.ShapeDtypeStruct((rows, width), blocks[0].dtype) for width in widths],
        in_specs=[WHOLE] * len(blocks) + [ANY],
        out_specs=[WHOLE] * len(widths),
        compiler_params=limits(8),
        cost_estimate=cost(2e8, 1e6),
        name="stack_blocks",
    )(*blocks, after)


def up_pairs(wg, wu, out, which, first=0):
    count, width, hidden = out.shape[0], out.shape[1], wg.shape[2]
    rows = pl.ds(pl.multiple_of((lax.axis_index("tp") ^ which) * width, 128), width)
    pairs = []
    for e in range(count):
        pairs.append((wg.at[first + e, rows, :], out.at[e, :, pl.ds(0, hidden)]))
        pairs.append((wu.at[first + e, rows, :], out.at[e, :, pl.ds(hidden, hidden)]))
    return pairs


def down_pairs(wd, out, which):
    local, depth, width = wd.shape[0], wd.shape[1], out.shape[1]
    columns = pl.ds(pl.multiple_of((lax.axis_index("tp") ^ which) * width, 128), width)
    return [(wd.at[e, :, columns], out.at[pl.ds(e * depth, depth), :]) for e in range(local)]


def hold_up_kernel(wg, wu, after, near_x, near_y, sems):
    pairs = up_pairs(wg, wu, near_x, 1) + up_pairs(wg, wu, near_y, 2)
    wait_all(start_all(pairs, sems))


def hold_up(w_gate, w_up, width, after):
    local, columns = w_gate.shape[0], 2 * w_gate.shape[2]
    return pl.pallas_call(
        hold_up_kernel,
        out_shape=[
            jax.ShapeDtypeStruct((local, width, columns), BF16),
            jax.ShapeDtypeStruct((local // 2, width, columns), BF16),
        ],
        in_specs=[ANY] * 3,
        out_specs=[WHOLE] * 2,
        scratch_shapes=[pltpu.SemaphoreType.DMA((3 * local,))],
        compiler_params=limits(2),
        cost_estimate=cost(5e9, 3.4e7),
        name="hold_up",
    )(in_hbm(w_gate), in_hbm(w_up), after)


def first_kernel(
    chips, slots, local, xm, xt, mm, mt, wg, wu, acc, sel, back, weight, near_y, buf,
    own_sems, sems,
):
    pairs = up_pairs(wg, wu, buf, 0)
    start_all(pairs, own_sems)
    others = start_all(up_pairs(wg, wu, near_y, 2, local - near_y.shape[0]), sems)
    per_block, half = 2 * chips * CAP, chips * slots
    core = (lax.axis_index("ep") & 1).astype(F32)
    unit = one_if(iota((16, META), 0) == iota((16, META), 1))
    total = jnp.zeros((local * per_block, 1), F32)
    for side, meta_ref in ((0, mm), (1, mt)):
        meta = meta_ref[...]
        turned = dot_nt(unit, meta)
        cols = meta.astype(F32)

        def slot_of(take, block, k):
            expert = take(2 * k) - 1.0 - core * local
            inside = (expert >= 0.0) & (expert < local)
            return jnp.where(inside, expert * per_block + block * CAP + take(2 * k + 1), -1.0)

        def block_of(shape, dim):
            place = iota(shape, dim)
            block = jnp.full(shape, side * chips, jnp.int32)
            for k in range(1, chips):
                block = block + jnp.where(place >= k * slots, 1, 0)
            return block.astype(F32)

        def row_value(k):
            return turned[k : k + 1, :]

        def col_value(k):
            return cols[:, k : k + 1]

        places = iota((local * per_block, half), 0).astype(F32)
        hits = [places == slot_of(row_value, block_of((1, half), 1), k) for k in range(TOP)]
        for k in range(TOP):
            base = 2 * TOP + 3 * k
            share = row_value(base) + row_value(base + 1) + row_value(base + 2)
            total += jnp.sum(jnp.where(hits[k], share, 0.0), axis=-1, keepdims=True)
        sel[side] = one_if(hits[0] | hits[1])
        wanted = [slot_of(col_value, block_of((half, 1), 0), k) for k in range(TOP)]
        lanes = iota((half, local * per_block), 1).astype(F32)
        back[side] = one_if((lanes == wanted[0]) | (lanes == wanted[1]))
    weight[...] = jnp.broadcast_to(total, weight.shape)

    @pl.loop(0, local)
    def _(e):
        picked = picked_rows(sel, e, per_block, xm, xt)
        for j in range(2):
            pltpu.make_async_copy(*pairs[j], own_sems.at[2 * e + j]).wait()
        acc[e] = dot(picked, buf[e])

    wait_all(others)


def picked_rows(sel, e, count, mine, twin):
    own = pl.ds(pl.multiple_of(e * count, 16), count)
    return (dot(sel[0, own, :], mine[...]) + dot(sel[1, own, :], twin[...])).astype(BF16)


def first_quarter(xm, xt, mm, mt, w_gate, w_up, chips, slots):
    local, hidden, width = w_gate.shape[0], w_gate.shape[2], xm.shape[1]
    per_block, half = 2 * chips * CAP, chips * slots
    shapes = [
        jax.ShapeDtypeStruct((local, per_block, 2 * hidden), F32),
        jax.ShapeDtypeStruct((2, local * per_block, half), BF16),
        jax.ShapeDtypeStruct((2, half, local * per_block), BF16),
        jax.ShapeDtypeStruct((local * per_block, META), F32),
        jax.ShapeDtypeStruct((local - local // 2, width, 2 * hidden), BF16),
    ]
    return pl.pallas_call(
        functools.partial(first_kernel, chips, slots, local),
        out_shape=shapes,
        in_specs=[WHOLE] * 4 + [ANY] * 2,
        out_specs=[WHOLE] * 5,
        scratch_shapes=[
            pltpu.VMEM((local, width, 2 * hidden), BF16),
            pltpu.SemaphoreType.DMA((2 * local,)),
            pltpu.SemaphoreType.DMA((2 * (local - local // 2),)),
        ],
        compiler_params=limits(12),
        cost_estimate=cost(3e9, 1e7),
        name="first_quarter",
    )(xm, xt, mm, mt, in_hbm(w_gate), in_hbm(w_up))


def beside_kernel(xm, xt, ym, yt, sel, start, near_x, low_y, high_y, wg, wu, wd, acc, far, down, *sems):
    copies = start_all(up_pairs(wg, wu, far, 3), sems[0])
    copies += start_all(down_pairs(wd, down, 3), sems[1])
    _, per_block = start.shape[:2]
    count = low_y.shape[0]

    @pl.loop(0, count)
    def _(i):
        for e, y_ref in ((i, low_y), (i + count, high_y)):
            both = start[e] + dot(picked_rows(sel, e, per_block, xm, xt), near_x[e])
            acc[e] = both + dot(picked_rows(sel, e, per_block, ym, yt), y_ref[i])

    wait_all(copies)


def beside_quarters(xm, xt, ym, yt, sel, start, near_x, low_y, high_y, w_gate, w_up, w_down):
    local, width = near_x.shape[:2]
    return pl.pallas_call(
        beside_kernel,
        out_shape=[
            jax.ShapeDtypeStruct(start.shape, F32),
            jax.ShapeDtypeStruct(near_x.shape, BF16),
            jax.ShapeDtypeStruct((local * w_down.shape[1], width), BF16),
        ],
        in_specs=[WHOLE] * 9 + [ANY] * 3,
        out_specs=[WHOLE] * 3,
        scratch_shapes=[
            pltpu.SemaphoreType.DMA((2 * local,)),
            pltpu.SemaphoreType.DMA((local,)),
        ],
        compiler_params=limits(4),
        cost_estimate=cost(3e9, 1e7),
        name="beside_quarters",
    )(
        xm, xt, ym, yt, sel, start, near_x, low_y, high_y, in_hbm(w_gate), in_hbm(w_up),
        in_hbm(w_down),
    )


def far_kernel(m0, m1, t0, t1, sel, weight, start, far, wd, out, down_x, down_y, xm, xt, *sems):
    copies = start_all(down_pairs(wd, down_x, 1), sems[0])
    copies += start_all(down_pairs(wd, down_y, 2), sems[1])
    local, hidden = start.shape[0], start.shape[2] // 2
    per_block, half = start.shape[1], sel.shape[2]
    for whole, parts in ((xm, (m0, m1)), (xt, (t0, t1))):
        whole[: half // 2, :] = parts[0][...]
        whole[half // 2 :, :] = parts[1][...]

    @pl.loop(0, local // 2)
    def _(i):
        for e in (2 * i, 2 * i + 1):
            mine = pl.ds(pl.multiple_of(e * per_block, 16), per_block)
            both = start[e] + dot(picked_rows(sel, e, per_block, xm, xt), far[e])
            gate = both[:, :hidden]
            act = gate / (1.0 + jnp.exp(-gate)) * both[:, hidden:] * weight[mine, 0:1]
            out[mine, :] = act.astype(BF16)

    wait_all(copies)


def far_quarter(m0, m1, t0, t1, sel, weight, start, far, w_down):
    local, hidden, width, half = start.shape[0], start.shape[2] // 2, m0.shape[1], sel.shape[2]
    down = jax.ShapeDtypeStruct((local * w_down.shape[1], width), BF16)
    return pl.pallas_call(
        far_kernel,
        out_shape=[jax.ShapeDtypeStruct((sel.shape[1], hidden), BF16), down, down],
        in_specs=[WHOLE] * 8 + [ANY],
        out_specs=[WHOLE] * 3,
        scratch_shapes=[pltpu.VMEM((half, width), BF16)] * 2
        + [pltpu.SemaphoreType.DMA((local,))] * 2,
        compiler_params=limits(6),
        cost_estimate=cost(3e9, 1e7),
        name="far_quarter",
    )(m0, m1, t0, t1, sel, weight, start, far, in_hbm(w_down))


def split_kernel(x_ref, y_ref, first, second):
    rows = first.shape[0]
    first[...] = x_ref[:rows, :]
    second[...] = y_ref[rows:, :]


def split_halves(x_block, y_block):
    half = jax.ShapeDtypeStruct((x_block.shape[0] // 2, x_block.shape[1]), BF16)
    return pl.pallas_call(
        split_kernel,
        out_shape=[half, half],
        in_specs=[WHOLE] * 2,
        out_specs=[WHOLE] * 2,
        compiler_params=limits(4),
        cost_estimate=cost(1e8, 1e6),
        name="split_halves",
    )(x_block, y_block)


def down_kernel(local, acts, back, wd, mine, twin, held):
    count, depth = acts.shape[0] // local, acts.shape[1]
    for e in range(local):
        rows = pl.ds(e * count, count)
        held[rows, :] = dot(acts[rows, :], wd[e * depth : (e + 1) * depth, :]).astype(BF16)
    twin[...] = dot(back[1], held[...]).astype(BF16)
    mine[...] = dot(back[0], held[...])


def down_quarter(acts, back, wd):
    half, width = back.shape[1], wd.shape[1]
    return pl.pallas_call(
        functools.partial(down_kernel, wd.shape[0] // acts.shape[1]),
        out_shape=[
            jax.ShapeDtypeStruct((half, width), F32),
            jax.ShapeDtypeStruct((half, width), BF16),
        ],
        in_specs=[WHOLE] * 3,
        out_specs=[WHOLE] * 2,
        scratch_shapes=[pltpu.VMEM((acts.shape[0], width), BF16)],
        compiler_params=limits(4),
        cost_estimate=cost(1.8e9, 6e6),
        name="down_quarter",
    )(acts, back, wd)


def sum_kernel(first, mine, twin, *refs):
    extras, out = refs[:-1], refs[-1]
    rows = pl.ds(first, out.shape[0])
    total = mine[rows, :] + twin[rows, :].astype(F32)
    for extra in extras:
        total += extra[...].astype(F32)
    out[...] = total.astype(BF16)


def sum_half(second, mine, twin, *extras):
    rows = mine.shape[0] // 2
    return pl.pallas_call(
        functools.partial(sum_kernel, rows * second),
        out_shape=jax.ShapeDtypeStruct((rows, mine.shape[1]), BF16),
        in_specs=[WHOLE] * (2 + len(extras)),
        out_specs=WHOLE,
        compiler_params=limits(4),
        cost_estimate=cost(2e8, 1e6),
        name="sum_half",
    )(mine, twin, *extras)


def join_kernel(first, slots, own, twin, x_part, y_part, *outs):
    for k, out in enumerate(outs):
        near = pl.ds(k * slots, slots)
        rows = pl.ds(first + k * slots, slots)
        total = own[rows, :] + twin[rows, :].astype(F32)
        out[...] = (total + x_part[near, :].astype(F32) + y_part[near, :].astype(F32)).astype(BF16)


def join_half(second, own, twin, x_part, y_part, slots):
    rows, width = x_part.shape
    return pl.pallas_call(
        functools.partial(join_kernel, second * rows, slots),
        out_shape=[jax.ShapeDtypeStruct((slots, width), BF16)] * (rows // slots),
        in_specs=[WHOLE] * 4,
        out_specs=[WHOLE] * (rows // slots),
        compiler_params=limits(4),
        cost_estimate=cost(3e8, 2e6),
        name="join_half",
    )(own, twin, x_part, y_part)


def place_kernel(pick, *refs):
    blocks, out, held = refs[:-2], refs[-2], refs[-1]
    slots = blocks[0].shape[0]
    for k, block in enumerate(blocks):
        held[k * slots : (k + 1) * slots, :] = block[...]
    out[...] = dot(pick[...], held[...]).astype(BF16)


def place_rows(pick, blocks):
    width = blocks[0].shape[1]
    return pl.pallas_call(
        place_kernel,
        out_shape=jax.ShapeDtypeStruct((pick.shape[0], width), BF16),
        in_specs=[WHOLE] * (1 + len(blocks)),
        out_specs=WHOLE,
        scratch_shapes=[pltpu.VMEM((pick.shape[1], width), BF16)],
        compiler_params=limits(16),
        cost_estimate=cost(5e8, 1e6),
        name="place_rows",
    )(pick, *blocks)


def head_masks(heads, shape):
    lanes = iota(shape, 1)
    edge = heads * NOPE
    masks = []
    for h in range(heads):
        nope = (lanes >= h * NOPE) & (lanes < (h + 1) * NOPE)
        turned = (lanes >= edge + h * ROPE) & (lanes < edge + (h + 1) * ROPE)
        masks.append(nope | turned)
    return masks


def attend_prep_kernel(heads, count, *refs):
    sources, (after, kv, stacked) = refs[:count], refs[count : count + 3]
    held, sems = refs[count + 3 : -1], refs[-1]
    for copy in start_all(list(zip(sources, held)), sems):
        copy.wait()
    latent, rope, lat_gain, key_up, value_up, queries, q_gain, k_gain, rates, q_map, k_map, g_map = held
    nope, turned = heads * NOPE, heads * ROPE
    rows = latent.shape[0]
    position = iota((rows, turned), 0) + lax.axis_index("ep") * rows
    angles = position.astype(F32) * rates[...]
    cos, sin = jnp.cos(angles), jnp.sin(angles)
    masks = head_masks(heads, (rows, nope + turned))
    place = iota((8, QKD), 0)
    split = jnp.zeros((8, QKD), F32)
    for i, gain in enumerate((q_gain, k_gain)):
        whole = gain[...]
        high = whole.astype(BF16).astype(F32)
        middle = (whole - high).astype(BF16).astype(F32)
        for j, piece in enumerate((high, middle, whole - high - middle)):
            split = jnp.where(place == 3 * i + j, piece, split)
    spread = dot(split.astype(BF16), g_map[...])
    gains = [spread[i : i + 1] + spread[i + 1 : i + 2] + spread[i + 2 : i + 3] for i in (0, 3)]

    def finish(values, pair, inverse, gain):
        low = values[:, :nope] * inverse[:, :nope] * gain[:, :nope]
        high = values[:, nope:] * gain[:, nope : nope + turned] * cos
        high = (high + pair * gain[:, nope + turned :] * sin) * inverse[:, nope:]
        return low, high

    both = dot(queries[...], q_map[...])
    values, pair = both[:, : nope + turned], both[:, nope + turned :]
    squares = values * values
    inverse = jnp.zeros(values.shape, F32)
    for mask in masks:
        total = jnp.sum(jnp.where(mask, squares, 0.0), axis=-1, keepdims=True)
        inverse = jnp.where(mask, lax.rsqrt(total / QKD + EPS), inverse)
    low, high = finish(values, pair, inverse, gains[0])
    for h in range(heads):
        mine = pl.ds(h * rows, rows)
        stacked[mine, :nope] = jnp.where(masks[h][:, :nope], low, 0.0).astype(BF16)
        stacked[mine, nope:] = jnp.where(masks[h][:, nope:], high, 0.0).astype(BF16)

    lat = latent[...].astype(F32)
    scale = lax.rsqrt(jnp.mean(lat * lat, axis=-1, keepdims=True) + EPS)
    normed = (lat * scale * lat_gain[...]).astype(BF16)
    key_nope = dot(normed, key_up[...]).astype(BF16).astype(F32)
    shared = lax.dot_general(
        rope[...], k_map[...], (((0,), (0,)), ((), ())), preferred_element_type=F32
    )
    turned_k, pair_k = shared[:, :turned], shared[:, turned:]
    values = jnp.concatenate([key_nope, turned_k], axis=1)
    squares = values * values
    inverse = jnp.zeros(values.shape, F32)
    for mask in masks:
        total = jnp.sum(jnp.where(mask, squares, 0.0), axis=-1, keepdims=True)
        inverse = jnp.where(mask, lax.rsqrt(total / QKD + EPS), inverse)
    low, high = finish(values, pair_k, inverse, gains[1])
    kv[:, :nope] = low.astype(BF16)
    kv[:, nope : nope + turned] = high.astype(BF16)
    kv[:, nope + turned :] = dot(normed, value_up[...]).astype(BF16)


def rope_maps(heads):
    half = ROPE // 2
    nope, turned = heads * NOPE, heads * ROPE
    q_map = np.zeros((heads * QKD, nope + 2 * turned), np.float32)
    k_map = np.zeros((ROPE, 2 * turned), np.float32)
    g_map = np.zeros((QKD, nope + 2 * turned), np.float32)
    for h in range(heads):
        for i in range(NOPE):
            q_map[h * QKD + i, h * NOPE + i] = 1
        for i in range(ROPE):
            other, sign = (i + half, -1) if i < half else (i - half, 1)
            at = h * ROPE + i
            q_map[h * QKD + NOPE + i, nope + at] = 1
            q_map[h * QKD + NOPE + other, nope + turned + at] = sign
            k_map[i, at] = 1
            k_map[other, turned + at] = sign
        g_map += np.abs(q_map[h * QKD : (h + 1) * QKD])
    rates = np.tile(np.float32(THETA) ** (-np.arange(half, dtype=np.float32) / half), turned // half)
    return [jnp.asarray(rates[None], F32)] + [jnp.asarray(m, BF16) for m in (q_map, k_map, g_map)]


def attend_prep(latent, rope, lat_gain, key_up, value_up, queries, query_gain, key_gain, after):
    rows, heads = latent.shape[0], key_up.shape[1] // NOPE
    wide = heads * (NOPE + ROPE)
    arrays = [latent, rope.T, lat_gain[None], key_up, value_up, queries]
    arrays += [query_gain[None], key_gain[None]] + rope_maps(heads)
    return pl.pallas_call(
        functools.partial(attend_prep_kernel, heads, len(arrays)),
        out_shape=[
            jax.ShapeDtypeStruct((rows, wide + heads * VDIM), BF16),
            jax.ShapeDtypeStruct((heads * rows, wide), BF16),
        ],
        in_specs=[ANY] * (len(arrays) + 1),
        out_specs=[WHOLE] * 2,
        scratch_shapes=scratch_like(*arrays),
        compiler_params=limits(8),
        cost_estimate=cost(2e9, 4e6),
        name="attend_prep",
    )(*[in_hbm(a) for a in arrays], after)


def attend_kernel(heads, chips, stacked, mine, twin, wd, out, down, held, mixed, sems):
    copies = start_all(down_pairs(wd, down, 0), sems)
    rows = out.shape[0]
    width = heads * (NOPE + ROPE)
    core = lax.axis_index("ep") & 1
    chip = lax.shift_right_logical(lax.axis_index("ep"), 1)
    place = iota((heads * rows, 1), 0)
    for h in range(1, heads):
        place = place - jnp.where(iota((heads * rows, 1), 0) >= h * rows, rows, 0)
    query_pos = place + lax.axis_index("ep") * rows

    @pl.loop(0, chips)
    def _(back):
        where = pl.ds(pl.multiple_of(back * rows, 128), rows)
        for side, keys in ((0, mine), (1, twin)):
            source = (chip - back) * 2 + (core if side == 0 else 1 - core)
            first = jnp.where(chip >= back, source * rows, 1 << 30)
            scores = dot_nt(stacked[...], keys[where, :width]) * (QKD ** (-0.5))
            seen = iota((heads * rows, rows), 1) + first <= query_pos
            lanes = pl.ds(pl.multiple_of((side * chips + back) * rows, 128), rows)
            held[:, lanes] = jnp.where(seen, scores, -1e30)

    mixed[...] = jnp.zeros(mixed.shape, F32)
    size = chips * rows
    lanes = iota((rows, heads * VDIM), 1)

    @pl.loop(0, heads // 2)
    def _(i):
        for h in (2 * i, 2 * i + 1):
            scores = held[pl.ds(pl.multiple_of(h * rows, 128), rows), :]
            expo = jnp.exp(scores - jnp.max(scores, axis=-1, keepdims=True))
            total = jnp.sum(expo, axis=-1, keepdims=True)
            probs = expo.astype(BF16)
            result = dot(probs[:, :size], mine[:, width:]) + dot(probs[:, size:], twin[:, width:])
            own = (lanes >= h * VDIM) & (lanes < (h + 1) * VDIM)
            mixed[...] += jnp.where(own, result / total, 0.0)

    out[...] = mixed[...].astype(BF16)
    wait_all(copies)


def attend(stacked, mine, twin, w_down, width, heads, chips):
    rows, local = stacked.shape[0] // heads, w_down.shape[0]
    return pl.pallas_call(
        functools.partial(attend_kernel, heads, chips),
        out_shape=[
            jax.ShapeDtypeStruct((rows, heads * VDIM), BF16),
            jax.ShapeDtypeStruct((local * w_down.shape[1], width), BF16),
        ],
        in_specs=[WHOLE] * 3 + [ANY],
        out_specs=[WHOLE] * 2,
        scratch_shapes=[
            pltpu.VMEM((heads * rows, 2 * chips * rows), F32),
            pltpu.VMEM((rows, heads * VDIM), F32),
            pltpu.SemaphoreType.DMA((local,)),
        ],
        compiler_params=limits(12),
        cost_estimate=cost(5e9, 4e6),
        name="attend",
    )(stacked, mine, twin, in_hbm(w_down))


def project_kernel(gain, proj, pair, far_pair, out):
    count, depth = out.shape[0], pair.shape[1]
    total = jnp.zeros(out.shape, F32)
    squares = jnp.zeros((count, 1), F32)
    for j in range(4):
        rows = pl.ds(pl.multiple_of((lax.axis_index("tp") ^ j) * depth, 128), depth)
        near = pl.ds((j & 1) * count, count)
        value = (pair if j < 2 else far_pair)[near, :].astype(F32)
        squares += jnp.sum(value * value, axis=-1, keepdims=True)
        total += dot((value * gain[:, rows]).astype(BF16), proj[rows, :])
    out[...] = (total * lax.rsqrt(squares / gain.shape[1] + EPS)).astype(BF16)


def project(gain, proj, pair, far_pair):
    return pl.pallas_call(
        project_kernel,
        out_shape=jax.ShapeDtypeStruct((pair.shape[0] // 2, proj.shape[1]), BF16),
        in_specs=[WHOLE] * 4,
        out_specs=WHOLE,
        compiler_params=limits(16),
        cost_estimate=cost(1e9, 3e6),
        name="project",
    )(gain[None], proj, pair, far_pair)


def twin_shards(
    queries, kv_latent, rope_key, latent_gain, key_up, value_up, query_gain, key_gain, out_gain,
    out_proj, moe_input, moe_gain, expert_ids, route_weights, w_gate, w_up, w_down,
):
    ep, tp = lax.axis_size("ep"), lax.axis_size("tp")
    chips, experts = ep // 2, ep * w_gate.shape[0]
    slots = PER_GROUP * CAP // TOP
    width = moe_input.shape[1] // tp
    heads = key_up.shape[1] // NOPE

    def send(values, axis, pairs):
        return lax.ppermute(values, axis, pairs)

    def along(values, shift):
        return send(values, "ep", [(i, (i + 2 * shift) % ep) for i in range(ep)])

    def across(values):
        return send(values, "ep", [(i, i ^ 1) for i in range(ep)])

    def sideways(values, which):
        return send(values, "tp", [(i, i ^ which) for i in range(tp)])

    others, middle = range(1, chips), chips // 2
    sources, pick = make_dispatch(
        moe_input, moe_gain, expert_ids, route_weights, chips, experts, slots, width
    )
    arrived = [sources[0]] + [along(sources[k], k) for k in others]
    near_x, low_y = hold_up(w_gate, w_up, width, pick)
    kv, stacked = attend_prep(
        kv_latent, rope_key, latent_gain, key_up, value_up, queries, query_gain,
        key_gain, pick,
    )
    own, meta = stack_blocks(arrived, (width, META), near_x)
    x_block, y_block = sideways(own, 1), sideways(own, 2)
    own_twin, meta_twin = across(own), across(meta)
    kv_blocks = [kv] + [along(kv, k) for k in others]
    start, sel, back, weight, high_y = first_quarter(
        own, own_twin, meta, meta_twin, w_gate, w_up, chips, slots
    )
    x_twin, y_twin = across(x_block), across(y_block)
    x_half, y_half = split_halves(x_block, y_block)
    far_first, far_second = sideways(x_half, 2), sideways(y_half, 1)
    start, far_weights, down_d = beside_quarters(
        x_block, x_twin, y_block, y_twin, sel, start, near_x, low_y, high_y,
        w_gate, w_up, w_down,
    )
    twin_first, twin_second = across(far_first), across(far_second)
    (kv_mine,) = stack_blocks(kv_blocks, (kv.shape[1],), kv)
    kv_twin = across(kv_mine)
    acts, down_x, down_y = far_quarter(
        far_first, far_second, twin_first, twin_second, sel, weight, start,
        far_weights, w_down,
    )
    d_mine, d_twin = down_quarter(acts, back, down_d)
    d_twin = across(d_twin)
    x_mine, x_twin = down_quarter(acts, back, down_x)
    x_twin = across(x_twin)
    from_y = sideways(sum_half(1, d_mine, d_twin), 2)
    from_x = sideways(sum_half(0, d_mine, d_twin), 1)
    y_mine, y_twin = down_quarter(acts, back, down_y)
    y_twin = across(y_twin)
    x_first = sideways(sum_half(0, x_mine, x_twin), 1)
    y_second = sideways(sum_half(1, y_mine, y_twin), 2)
    x_second = sideways(sum_half(1, x_mine, x_twin, from_y), 1)
    y_first = sideways(sum_half(0, y_mine, y_twin, from_x), 2)
    attn, down_own = attend(stacked, kv_mine, kv_twin, w_down, width, heads, chips)
    mine, twin = down_quarter(acts, back, down_own)
    twin = across(twin)
    attn_x = sideways(attn, 1)
    second = join_half(1, mine, twin, x_second, y_second, slots)
    returned = [along(block, -k) for k, block in enumerate(second, middle)]
    (pair,) = stack_blocks([attn, attn_x], (attn.shape[1],), kv)
    far_pair = sideways(pair, 2)
    first = join_half(0, mine, twin, x_first, y_first, slots)
    returned = [along(first[k], -k) for k in range(1, middle)] + returned
    mixed = project(out_gain, out_proj, pair, far_pair)
    expert_out = place_rows(pick, [first[0]] + returned)
    return (mixed, expert_out)


def fits_twins(mesh, w_gate):
    ep, tp = mesh.shape["ep"], mesh.shape["tp"]
    local = w_gate.shape[0] // ep
    return tp == 4 and ep % 4 == 0 and local % 2 == 0 and 2 * local == PER_GROUP and w_gate.shape[0] + ep // 2 <= META


def solution(mesh):
    in_specs = (
        P("ep", "tp"),
        P("ep", None),
        P("ep", None),
        P(),
        P(None, "tp"),
        P(None, "tp"),
        P(),
        P(),
        P(),
        P(None, "tp"),
        P("ep", None),
        P(),
        P("ep", None),
        P("ep", None),
        P("ep", None, "tp"),
        P("ep", None, "tp"),
        P("ep", "tp", None),
    )
    out_specs = (P("ep", "tp"), P("ep", "tp"))

    def mapped(body):
        return jax.shard_map(
            body, mesh=mesh, in_specs=in_specs, out_specs=out_specs, check_vma=False
        )

    def step(*arrays):
        if not fits_twins(mesh, arrays[14]):
            return mapped(shards)(*arrays)
        return mapped(twin_shards)(*arrays)

    return step
```
